32 devices in a mesh: sp: 16 (over z, y, x), tp: 2 (over core).
Axes of the slice: x: 2, y: 2, z: 4, core: 2. Of those that a mesh axis runs over, the one named last changes fastest.
Arguments:
- hidden_in: bfloat16 [4096, 2048], P('sp'), may hold values from -16 to 16
- query_one: bfloat16 [2048, 512], P(None, 'tp'), may hold values from -0.13258252 to 0.13258252
- query_two: bfloat16 [2048, 512], P(None, 'tp'), may hold values from -0.13258252 to 0.13258252
- key_one: bfloat16 [2048, 512], P(None, 'tp'), may hold values from -0.13258252 to 0.13258252
- key_two: bfloat16 [2048, 512], P(None, 'tp'), may hold values from -0.13258252 to 0.13258252
- value_proj: bfloat16 [2048, 1024], P(None, 'tp'), may hold values from -0.125 to 0.125
- lambdas: float32 [8], P('tp'), may hold values from 0.3 to 0.8
- norm_gain: float32 [128], replicated, may hold values from 0.1 to 1.9
- out_proj: bfloat16 [1024, 2048], P('tp'), may hold values from -0.1875 to 0.1875
Outputs:
- attended: bfloat16 [4096, 2048], P('sp')
The draws below stay inside these ranges and needn't reach their ends.
All inputs are finite; a program needn't handle non-finite values.
Results may differ from the reference program's by a relative error of at most 0.015.
Values may be sent and summed in bfloat16 or wider, within the bound.
A program may use at most 64 MiB of HBM per device.

```python
import math
import jax
import jax.numpy as jnp
from jax import lax

D = 2048
HEADS = 8
HEAD_QK = 64
HEAD_V = 128
TOK_DEV = 256
TOKENS = 4096
N_TP = 2


def draw_hidden_in(key, part):
    blocks = TOKENS // TOK_DEV
    noise_key = jax.random.fold_in(key, 101)
    shift_key = jax.random.fold_in(key, 102)
    offsets = 0.6 * jax.random.normal(shift_key, (blocks, 1, D), jnp.float32)
    base = 0.8 * jax.random.normal(noise_key, (blocks, TOK_DEV, D), jnp.float32)
    field = base + offsets
    return jnp.clip(field.reshape(TOKENS, D), -16.0, 16.0).astype(jnp.bfloat16)


def plain_weight(key, salt):
    base = jax.random.normal(jax.random.fold_in(key, salt), (D, HEADS * HEAD_QK), jnp.float32)
    return jnp.clip(base, -6.0, 6.0) * D ** (-0.5)


def draw_query_one(key, part):
    return plain_weight(key, 201).astype(jnp.bfloat16)


def draw_query_two(key, part):
    return plain_weight(key, 301).astype(jnp.bfloat16)


def draw_key_one(key, part):
    return plain_weight(key, 211).astype(jnp.bfloat16)


def draw_key_two(key, part):
    return plain_weight(key, 311).astype(jnp.bfloat16)


def shard_levels(rng, dims, split, least, high):
    loudness = 1.0
    for dim, blocks in split:
        draws = jax.random.uniform(jax.random.fold_in(jax.random.fold_in(rng, 6), dim), (blocks,), jnp.float32, least / len(split), high / len(split))
        loudness = loudness * jnp.repeat(jnp.exp(draws), dims[dim] // blocks).reshape((-1,) + (1,) * (len(dims) - 1 - dim))
    return loudness


def scatter_about(key, dims, spread, bound, split=(), held_as=jnp.bfloat16):
    array = jax.random.normal(key, dims, jnp.float32) * spread
    if len(split) > 0:
        array = shard_levels(key, dims, split, -0.22, 0.18) * array
    return jnp.clip(array, min=-bound, max=bound).astype(held_as)


def setup_inputs(seed: int = 0) -> dict:
    key_list = jax.random.split(jax.random.key(seed), 10)
    hidden_in = draw_hidden_in(jax.random.fold_in(key_list[9], 71), 0)
    query_one = draw_query_one(jax.random.fold_in(key_list[9], 71), 0)
    query_two = draw_query_two(jax.random.fold_in(key_list[9], 71), 0)
    key_one = draw_key_one(jax.random.fold_in(key_list[9], 71), 0)
    key_two = draw_key_two(jax.random.fold_in(key_list[9], 71), 0)
    value_proj = scatter_about(key_list[5], (D, HEADS * HEAD_V), D ** -0.5, 0.125, ((1, 2),))
    lambdas = jnp.clip(0.3 + 0.5 * jax.random.uniform(key_list[6], (HEADS,), jnp.float32) ** shard_levels(key_list[6], (HEADS,), ((0, 2),), -0.2, 0.2), 0.3, 0.8)
    norm_gain = jnp.clip(1.0 + 0.18 * jax.random.normal(key_list[7], (HEAD_V,), jnp.float32), 0.1, 1.9)
    out_proj = scatter_about(key_list[8], (HEADS * HEAD_V, D), (HEADS * HEAD_V) ** -0.5, 0.1875, ((0, 2),))
    return {"hidden_in": hidden_in, "query_one": query_one, "query_two": query_two, "key_one": key_one, "key_two": key_two, "value_proj": value_proj, "lambdas": lambdas, "norm_gain": norm_gain, "out_proj": out_proj}


epsilon = 1e-06
masked_score = -1e+30

def reference(hidden_in, query_one, query_two, key_one, key_two, value_proj, lambdas, norm_gain, out_proj):

    def project(weight, width):
        product = jnp.dot(hidden_in, weight, preferred_element_type=jnp.float32)
        return product.astype(jnp.bfloat16).reshape(TOKENS, HEADS, width)
    query_a = project(query_one, HEAD_QK)
    query_b = project(query_two, HEAD_QK)
    keys_a = project(key_one, HEAD_QK).astype(jnp.float32)
    keys_b = project(key_two, HEAD_QK).astype(jnp.float32)
    value_rows = project(value_proj, HEAD_V).astype(jnp.float32)
    score_scale = 1.75 * HEAD_QK ** (-0.5)
    key_pos = jnp.arange(TOKENS, dtype=jnp.int32)
    query_rows = math.gcd(TOKENS, 512)

    def one_block(block_index):
        begin = block_index * query_rows
        row_pos = begin + jnp.arange(query_rows, dtype=jnp.int32)
        allowed = key_pos[None, :] <= row_pos[:, None]

        def attend(queries, keys):
            chosen = lax.dynamic_slice_in_dim(queries, begin, query_rows, 0).astype(jnp.float32)
            scores = jnp.einsum('qhd,khd->hqk', chosen, keys) * score_scale
            scores = jnp.where(allowed[None], scores, masked_score)
            highest = lax.optimization_barrier(jnp.max(scores, axis=-1, keepdims=True))
            expos = jnp.where(allowed[None], jnp.exp(scores - highest), 0.0)
            summed = lax.optimization_barrier(jnp.sum(expos, axis=-1))
            rounded = lax.optimization_barrier(expos.astype(jnp.bfloat16))
            accum = jnp.einsum('hqk,khe->hqe', rounded.astype(jnp.float32), value_rows)
            return accum / summed[..., None]
        mixed_out = attend(query_a, keys_a) - lambdas[:, None, None] * attend(query_b, keys_b)
        scale_rows = lax.rsqrt(lax.optimization_barrier(jnp.mean(mixed_out * mixed_out, axis=-1, keepdims=True)) + epsilon)
        normed = (mixed_out * scale_rows * norm_gain).astype(jnp.bfloat16)
        return jnp.transpose(normed, (1, 0, 2)).reshape(query_rows, HEADS * HEAD_V)
    normed = lax.map(one_block, jnp.arange(TOKENS // query_rows, dtype=jnp.int32))
    normed = normed.reshape(TOKENS, HEADS * HEAD_V)
    group_cols = HEADS * HEAD_V // N_TP
    summed = jnp.zeros((TOKENS, D), jnp.float32)
    for group_index in range(N_TP):
        lower = group_index * group_cols
        part = jnp.dot(normed[:, lower:lower + group_cols], out_proj[lower:lower + group_cols], preferred_element_type=jnp.float32).astype(jnp.bfloat16)
        part = lax.optimization_barrier(part)
        summed = summed + part.astype(jnp.float32)
    return summed.astype(jnp.bfloat16)
```

```python
import math

import jax
import jax.numpy as jnp
from jax import lax
from jax.experimental import pallas as pl
from jax.experimental.pallas import tpu as pltpu
from jax.sharding import PartitionSpec as P

epsilon = 1e-06
masked_score = -1e30


def shards(
    hidden_in, query_one, query_two, key_one, key_two, value_proj, lambdas, norm_gain, out_proj
):
    heads_dev = lambdas.shape[0]
    head_qk = query_one.shape[1] // heads_dev
    head_v = value_proj.shape[1] // heads_dev
    width_q = heads_dev * head_qk
    score_scale = 1.75 * head_qk ** (-0.5)
    joined = jnp.concatenate((query_one, query_two, key_one, key_two, value_proj), axis=1)
    projected = jnp.dot(hidden_in, joined, preferred_element_type=jnp.float32).astype(jnp.bfloat16)
    tok_rows = projected.shape[0]
    key_values = projected[:, 2 * width_q :]
    my_index = lax.axis_index("sp")
    offset = my_index * tok_rows
    query_sets = (projected[:, : 2 * width_q],)
    position_sets = (offset + jnp.arange(tok_rows, dtype=jnp.int32),)
    groups = []
    for query_rows, positions in zip(query_sets, position_sets):
        group_rows = query_rows.shape[0]
        query_a = query_rows[:, :width_q].reshape(group_rows, heads_dev, head_qk)
        query_b = query_rows[:, width_q:].reshape(group_rows, heads_dev, head_qk)
        groups.append((query_a, query_b, positions, positions[group_rows - 1]))

    def one_map(queries, keys, value_rows, allowed, running_max, running_sum, accum):
        scores = (
            jnp.einsum("qhd,khd->hqk", queries, keys, preferred_element_type=jnp.float32)
            * score_scale
        )
        scores = jnp.where(allowed[None], scores, masked_score)
        new_max = jnp.maximum(running_max, jnp.max(scores, axis=-1))
        rescale = jnp.exp(running_max - new_max)
        weights = jnp.where(allowed[None], jnp.exp(scores - new_max[..., None]), 0.0)
        new_sum = running_sum * rescale + jnp.sum(weights, axis=-1)
        added = jnp.einsum(
            "hqk,khe->hqe",
            weights.astype(jnp.bfloat16),
            value_rows,
            preferred_element_type=jnp.float32,
        )
        return (new_max, new_sum, accum * rescale[..., None] + added)

    def absorb(group_state, group, kblock, kstart):
        query_a, query_b, positions, last_pos = group
        block_rows = kblock.shape[0]
        k_pos = kstart + jnp.arange(block_rows, dtype=jnp.int32)
        allowed = k_pos[None, :] <= positions[:, None]
        keys_a = kblock[:, :width_q].reshape(block_rows, heads_dev, head_qk)
        keys_b = kblock[:, width_q : 2 * width_q].reshape(block_rows, heads_dev, head_qk)
        value_rows = kblock[:, 2 * width_q :].reshape(block_rows, heads_dev, head_v)
        first_map = one_map(query_a, keys_a, value_rows, allowed, *group_state[:3])
        second_map = one_map(query_b, keys_b, value_rows, allowed, *group_state[3:])
        return first_map + second_map

    group = groups[0]
    group_rows = group[0].shape[0]
    start_max = jnp.full((heads_dev, group_rows), masked_score, jnp.float32)
    start_sum = jnp.zeros((heads_dev, group_rows), jnp.float32)
    start_acc = jnp.zeros((heads_dev, group_rows, head_v), jnp.float32)
    initial_list = [(start_max, start_sum, start_acc, start_max, start_sum, start_acc)]
    initial = tuple(initial_list)
    softmax_state = initial
    kv_piece = lax.all_gather(key_values, "sp", axis=0, tiled=True)
    piece_rows = kv_piece.shape[0]
    block_rows = math.gcd(piece_rows, 512)
    block_count = piece_rows // block_rows
    stacked = kv_piece.reshape(block_count, block_rows, kv_piece.shape[1])

    def absorb_step(carried, blocks_in):
        kblock, block_index = blocks_in
        kstart = block_index * block_rows
        renewed = []
        for group, group_state in zip(groups, carried):
            renewed.append(
                lax.cond(
                    kstart <= group[3],
                    lambda inner, group=group: absorb(inner, group, kblock, kstart),
                    lambda inner: inner,
                    group_state,
                )
            )
        return (tuple(renewed), None)

    softmax_state, _ = lax.scan(
        absorb_step, softmax_state, (stacked, jnp.arange(block_count, dtype=jnp.int32))
    )
    normed_sets = []
    for group_state in softmax_state:
        out_a = group_state[2] / group_state[1][..., None]
        out_b = group_state[5] / group_state[4][..., None]
        mixed_out = out_a - lambdas[:, None, None] * out_b
        scale_rows = lax.rsqrt(jnp.mean(mixed_out * mixed_out, axis=-1, keepdims=True) + epsilon)
        normed = (mixed_out * scale_rows * norm_gain).astype(jnp.bfloat16)
        group_rows = normed.shape[1]
        normed_sets.append(jnp.transpose(normed, (1, 0, 2)).reshape(group_rows, heads_dev * head_v))
    normed_all = normed_sets[0]
    partial_value = jnp.dot(normed_all, out_proj, preferred_element_type=jnp.float32)
    result = lax.psum(partial_value.astype(jnp.bfloat16), "tp")
    return result


MESH = pl.DeviceIdType.MESH
PLANE = 4
ROW_TILE = 256
OUT_TILE = 1024


def fused_kernel(
    groups,
    score_scale,
    hidden_hbm,
    q1_hbm,
    q2_hbm,
    k1_hbm,
    k2_hbm,
    v_hbm,
    lam_hbm,
    gain_hbm,
    wo_hbm,
    out_ref,
    hid,
    wq1,
    wq2,
    wk1,
    wk2,
    wv,
    wo,
    lam_ref,
    gain_ref,
    k_out,
    v_out,
    q_out,
    k_all,
    v_all,
    q_all,
    n_out,
    n_all,
    max_all,
    sum_all,
    acc_all,
    load_sem,
    wo_send,
    wo_recv,
    zk_send,
    zk_recv,
    zv_send,
    zv_recv,
    q_send,
    q_recv,
    xk_send,
    xk_recv,
    xv_send,
    xv_recv,
    yk_send,
    yk_recv,
    yv_send,
    yv_recv,
    fk_send,
    fk_recv,
    fv_send,
    fv_recv,
    n_send,
    n_recv,
    r_send,
    r_recv,
):
    scope = jax.named_scope
    me = lax.axis_index("sp")
    core = lax.axis_index("tp")
    plane = me // PLANE
    spot = lax.rem(me, PLANE)
    x_spot = spot + 1 - 2 * lax.rem(spot, 2)
    y_spot = spot + 2 - 4 * (spot // 2)
    rows = hid.shape[0]
    qk = q1_hbm.shape[1] // groups
    width = 2 * qk
    head_v = v_hbm.shape[1] // groups

    def load(index, src, dst):
        return pltpu.make_async_copy(src, dst, load_sem.at[index])

    loads = [
        load(0, hidden_hbm, hid),
        load(1, k1_hbm, wk1),
        load(2, k2_hbm, wk2),
        load(3, v_hbm, wv),
        load(4, q1_hbm, wq1),
        load(5, q2_hbm, wq2),
        load(6, wo_hbm, wo.at[core]),
        load(7, lam_hbm, lam_ref),
        load(8, gain_hbm, gain_ref),
    ]
    for item in loads:
        item.start()
    barrier = pltpu.get_barrier_semaphore()

    def greet(index, tp_index):
        pl.semaphore_signal(barrier, inc=1, device_id=(index, tp_index), device_id_type=MESH)

    for step in range(1, groups):
        other = lax.rem(plane + step, groups) * PLANE + spot
        greet(other, core)
    greet(me, 1 - core)
    greet(plane * PLANE + x_spot, core)
    greet(plane * PLANE + y_spot, core)

    pending = []

    def send(src, dst, send_sem, recv_sem, index, tp_index):
        return pltpu.make_async_remote_copy(
            src_ref=src,
            dst_ref=dst,
            send_sem=send_sem,
            recv_sem=recv_sem,
            device_id=(index, tp_index),
            device_id_type=MESH,
        )

    def begin(*args):
        copy = send(*args)
        copy.start()
        pending.append(copy)

    def arrived(ref, recv_sem):
        pltpu.make_async_copy(ref, ref, recv_sem).wait()

    upper = plane >= groups // 2
    mirrored = jnp.where(upper, groups - 1 - plane, plane)

    def from_plane(step):
        if step == 0:
            return plane
        near = jnp.where(step - 1 < mirrored, step - 1, step)
        return jnp.where(upper, groups - 1 - near, near)

    def project(weight_ref):
        return jnp.dot(hid[...], weight_ref[...], preferred_element_type=jnp.float32)

    def joined(first, second, store):
        for head in range(groups):
            cut = slice(head * qk, (head + 1) * qk)
            store(head, jnp.concatenate((first[:, cut], second[:, cut]), axis=1))

    outer = jnp.logical_or(plane == 0, plane == groups - 1)
    inner = jnp.logical_not(outer)

    def z_copy(kind, step):
        target = from_plane(step)
        out, full, sems, recvs = {
            "k": (k_out, k_all.at[me], zk_send, zk_recv),
            "v": (v_out, v_all.at[me], zv_send, zv_recv),
            "q": (q_out, q_all.at[plane], q_send, q_recv),
        }[kind]
        return send(
            out.at[target],
            full,
            sems.at[step],
            recvs.at[plane],
            target * PLANE + spot,
            core,
        )

    def z_start(*items):
        for kind, step in items:
            z_copy(kind, step).start()

    def z_done(*items):
        for kind, step in items:
            z_copy(kind, step).wait_send()

    far = [step for step in range(2, groups)]

    def gate(index):
        with scope(f"gate#{index}"):

            @pl.when(outer)
            def _():
                z_done(("v", index))
                if index < groups - 1:
                    z_start(("k", index + 1), ("v", index + 1))
                else:
                    z_start(*(("q", step) for step in far))

            if index < groups - 1:

                @pl.when(inner)
                def _():
                    z_done(("v", index + 1))
                    if index + 1 < groups - 1:
                        z_start(("k", index + 2), ("v", index + 2))
                    else:
                        z_start(*(("q", step) for step in far))

    def x_block(step):
        return from_plane(step) * PLANE + x_spot

    def y_block(step):
        return from_plane(step) * PLANE + y_spot

    def spread_k(step):
        slot = k_all.at[from_plane(step) * PLANE + spot]
        begin(slot, slot, xk_send.at[step], xk_recv.at[step], plane * PLANE + x_spot, core)
        begin(slot, slot, yk_send.at[step], yk_recv.at[step], plane * PLANE + y_spot, core)

    def spread_v(step):
        slot = v_all.at[from_plane(step) * PLANE + spot]
        begin(slot, slot, yv_send.at[step], yv_recv.at[step], plane * PLANE + y_spot, core)
        begin(slot, slot, xv_send.at[step], xv_recv.at[step], plane * PLANE + x_spot, core)

    def forward(step):
        source = from_plane(step)
        with scope(f"zk#s={step}"):
            arrived(k_all.at[source * PLANE + spot], zk_recv.at[source])
        spread_k(step)
        with scope(f"zv#s={step}"):
            arrived(v_all.at[source * PLANE + spot], zv_recv.at[source])
        spread_v(step)

    def relay(step):
        with scope(f"rk#s={step}"):
            slot = k_all.at[x_block(step)]
            arrived(slot, xk_recv.at[step])
        begin(slot, slot, fk_send.at[step], fk_recv.at[step], plane * PLANE + y_spot, core)
        with scope(f"rv#s={step}"):
            slot = v_all.at[y_block(step)]
            arrived(slot, yv_recv.at[step])
        begin(slot, slot, fv_send.at[step], fv_recv.at[step], plane * PLANE + x_spot, core)

    def ready(step):
        far = from_plane(step) * PLANE + (PLANE - 1 - spot)
        with scope(f"ready#s={step}"):
            arrived(v_all.at[x_block(step)], xv_recv.at[step])
            arrived(k_all.at[y_block(step)], yk_recv.at[step])
            arrived(k_all.at[far], fk_recv.at[step])
            arrived(v_all.at[far], fv_recv.at[step])

    def ready_q(step):
        with scope(f"q#s={step}"):
            slot = q_all.at[from_plane(step)]
            arrived(slot, q_recv.at[from_plane(step)])

    with scope("w_hid"):
        loads[0].wait()
    with scope("w_k"):
        loads[1].wait()
        loads[2].wait()
    with scope("p_k"):
        first = project(wk1).astype(jnp.bfloat16)
        second = project(wk2).astype(jnp.bfloat16)

        def put_k(head, value):
            k_out[head] = value

        joined(first, second, put_k)
        k_all[me] = k_out[plane]
    with scope("barrier"):
        pl.semaphore_wait(barrier, groups - 1 + 3)
    z_start(("k", 1))
    pl.when(inner)(lambda: z_start(("k", 2)))
    spread_k(0)
    with scope("w_v"):
        loads[3].wait()
    with scope("p_v"):
        value = project(wv).astype(jnp.bfloat16)
        for head in range(groups):
            v_out[head] = value[:, head * head_v : (head + 1) * head_v]
        v_all[me] = v_out[plane]
    z_start(("v", 1))
    pl.when(inner)(lambda: z_start(("v", 2)))
    spread_v(0)
    with scope("w_q"):
        loads[4].wait()
        loads[5].wait()
    with scope("p_q"):
        first = (project(wq1) * score_scale).astype(jnp.bfloat16)
        second = (project(wq2) * score_scale).astype(jnp.bfloat16)

        def put_q(head, value):
            q_out[head] = value

        joined(first, second, put_q)
        q_all[plane] = q_out[plane]
    z_start(("q", 1))
    loads[6].wait()
    begin(wo.at[core], wo.at[core], wo_send, wo_recv, me, 1 - core)
    loads[7].wait()
    loads[8].wait()

    tile = ROW_TILE
    tiles = rows // tile
    chunk = PLANE * rows
    lane = lax.broadcasted_iota(jnp.int32, (tile, width), 1)

    def pair_tile(group, key_group, part, diagonal):
        begin_row = pl.multiple_of(part * tile, tile)
        queries = q_all[group, pl.ds(begin_row, tile), :]
        zero = jnp.zeros_like(queries)
        both = jnp.concatenate(
            (jnp.where(lane < qk, queries, zero), jnp.where(lane >= qk, queries, zero)), axis=0
        )
        keys = k_all[pl.ds(key_group * PLANE, PLANE)].reshape(chunk, width)
        values = v_all[pl.ds(key_group * PLANE, PLANE)].reshape(chunk, head_v)
        scores = lax.dot_general(
            both, keys, (((1,), (1,)), ((), ())), preferred_element_type=jnp.float32
        )
        if diagonal:
            q_pos = (
                spot * rows
                + begin_row
                + lax.rem(lax.broadcasted_iota(jnp.int32, (2 * tile, chunk), 0), tile)
            )
            k_pos = lax.broadcasted_iota(jnp.int32, (2 * tile, chunk), 1)
            scores = jnp.where(k_pos <= q_pos, scores, masked_score)
        new_max = jnp.max(scores, axis=-1, keepdims=True)
        running_max = max_all[group, part]
        new_max = jnp.maximum(running_max, new_max)
        rescale = jnp.exp2(running_max - new_max)
        weights = jnp.exp2(scores - new_max)
        new_sum = jnp.sum(weights, axis=-1, keepdims=True)
        accum = jnp.dot(
            weights.astype(jnp.bfloat16), values, preferred_element_type=jnp.float32
        )
        max_all[group, part] = new_max
        sum_all[group, part] = sum_all[group, part] * rescale + new_sum
        acc_all[group, part] = acc_all[group, part] * rescale + accum

    def pair(group, key_group, diagonal):
        if not COMPUTE:
            return
        with scope("pair_d" if diagonal else "pair"):
            lax.fori_loop(
                0, tiles, lambda t, c: (pair_tile(group, key_group, t, diagonal), c)[1], 0
            )

    def meet(step, earlier):
        one, other = from_plane(step), from_plane(earlier)
        pair(jnp.maximum(one, other), jnp.minimum(one, other), False)

    def normed_copy(group):
        return send(
            n_out.at[group],
            n_all.at[core, plane],
            n_send.at[group],
            n_recv.at[plane],
            group * PLANE + spot,
            core,
        )

    def partner_copy(head):
        slot = n_all.at[core, head]
        return send(slot, slot, r_send.at[head], r_recv.at[head], me, 1 - core)

    lam = lam_ref[plane]
    gain = gain_ref[...]

    def finish(step):
        group = from_plane(step)
        if not COMPUTE:
            return

        def finish_tile(part, _):
            begin_row = pl.multiple_of(part * tile, tile)
            heads_out = acc_all[group, part] / sum_all[group, part]
            mixed = heads_out[:tile] - lam * heads_out[tile:]
            scale_rows = lax.rsqrt(jnp.mean(mixed * mixed, axis=-1, keepdims=True) + epsilon)
            normed = (mixed * scale_rows * gain).astype(jnp.bfloat16)
            n_out[group, pl.ds(begin_row, tile), :] = normed
            return 0

        lax.fori_loop(0, tiles, finish_tile, 0)

    def deliver(step):
        finish(step)
        group = from_plane(step)
        if step == 0:
            n_all[core, plane] = n_out[plane]
            partner_copy(plane).start()
        else:
            normed_copy(group).start()

    max_all[...] = jnp.full(max_all.shape, masked_score, jnp.float32)
    sum_all[...] = jnp.zeros(sum_all.shape, jnp.float32)
    acc_all[...] = jnp.zeros(acc_all.shape, jnp.float32)

    relay(0)
    gate(1)
    forward(1)
    ready(0)
    pair(plane, plane, True)
    forward(2)
    relay(1)
    gate(2)
    ready(1)
    ready_q(1)
    meet(1, 0)
    pair(from_plane(1), from_plane(1), True)
    relay(2)
    gate(3)
    forward(3)
    ready(2)
    ready_q(2)
    meet(2, 0)
    meet(2, 1)
    relay(3)
    pair(from_plane(2), from_plane(2), True)
    ready(3)
    ready_q(3)
    meet(3, 1)
    deliver(1)
    meet(3, 2)
    deliver(2)
    meet(3, 0)
    deliver(0)
    pair(from_plane(3), from_plane(3), True)
    deliver(3)

    for step in range(1, groups):
        head = from_plane(step)
        slot = n_all.at[core, head]
        with scope(f"n#s={step}"):
            arrived(slot, n_recv.at[head])
        partner_copy(head).start()

    def out_tiles(tp_index, first_part):
        normed = jnp.concatenate([n_all[tp_index, head] for head in range(groups)], axis=1)

        def out_tile(index, _):
            columns = pl.ds(pl.multiple_of(index * OUT_TILE, OUT_TILE), OUT_TILE)
            part = jnp.dot(normed, wo[tp_index, :, columns], preferred_element_type=jnp.float32)
            part = part.astype(jnp.bfloat16)
            if not first_part:
                part = (part.astype(jnp.float32) + out_ref[:, columns].astype(jnp.float32)).astype(
                    jnp.bfloat16
                )
            out_ref[:, columns] = part
            return 0

        lax.fori_loop(0, out_ref.shape[1] // OUT_TILE, out_tile, 0)

    with scope("out1"):
        out_tiles(core, True)
    with scope("rrecv"):
        arrived(wo.at[1 - core], wo_recv)
        for head in range(groups):
            arrived(n_all.at[1 - core, head], r_recv.at[head])
    with scope("out2"):
        out_tiles(1 - core, False)

    with scope("drain"):
        for copy in pending:
            copy.wait_send()
        pl.when(inner)(lambda: z_done(("v", 1)))
        for step in range(1, groups):
            z_done(("k", step), ("q", step))
            normed_copy(from_plane(step)).wait_send()
        for head in range(groups):
            partner_copy(head).wait_send()


COMPUTE = True


def fused_shards(
    hidden_in, query_one, query_two, key_one, key_two, value_proj, lambdas, norm_gain, out_proj
):
    groups = lambdas.shape[0]
    rows, depth = hidden_in.shape
    head_qk = query_one.shape[1] // groups
    head_v = value_proj.shape[1] // groups
    width = 2 * head_qk
    blocks = groups * PLANE
    columns = out_proj.shape[1]
    score_scale = 1.75 * head_qk ** (-0.5) * math.log2(math.e)
    bf16 = jnp.bfloat16
    dma = pltpu.SemaphoreType.DMA
    hbm = pl.BlockSpec(memory_space=pltpu.HBM)
    vmem = pl.BlockSpec(memory_space=pltpu.VMEM)

    def body(*refs):
        fused_kernel(groups, score_scale, *refs)

    return pl.pallas_call(
        body,
        name="fused_attention",
        out_shape=jax.ShapeDtypeStruct((rows, columns), bf16),
        in_specs=[hbm] * 9,
        out_specs=vmem,
        scratch_shapes=[
            pltpu.VMEM(hidden_in.shape, bf16),
            pltpu.VMEM(query_one.shape, bf16),
            pltpu.VMEM(query_two.shape, bf16),
            pltpu.VMEM(key_one.shape, bf16),
            pltpu.VMEM(key_two.shape, bf16),
            pltpu.VMEM(value_proj.shape, bf16),
            pltpu.VMEM((2,) + out_proj.shape, bf16),
            pltpu.SMEM(lambdas.shape, jnp.float32),
            pltpu.VMEM((1, head_v), jnp.float32),
            pltpu.VMEM((groups, rows, width), bf16),
            pltpu.VMEM((groups, rows, head_v), bf16),
            pltpu.VMEM((groups, rows, width), bf16),
            pltpu.VMEM((blocks, rows, width), bf16),
            pltpu.VMEM((blocks, rows, head_v), bf16),
            pltpu.VMEM((groups, rows, width), bf16),
            pltpu.VMEM((groups, rows, head_v), bf16),
            pltpu.VMEM((2, groups, rows, head_v), bf16),
            pltpu.VMEM((groups, rows // ROW_TILE, 2 * ROW_TILE, 1), jnp.float32),
            pltpu.VMEM((groups, rows // ROW_TILE, 2 * ROW_TILE, 1), jnp.float32),
            pltpu.VMEM((groups, rows // ROW_TILE, 2 * ROW_TILE, head_v), jnp.float32),
            dma((9,)),
            dma,
            dma,
        ]
        + [dma((groups,))] * 22,
        compiler_params=pltpu.CompilerParams(
            collective_id=0, has_side_effects=True, vmem_limit_bytes=VMEM_LIMIT
        ),
    )(
        *(
            pltpu.with_memory_space_constraint(item, pltpu.HBM)
            for item in (
                hidden_in,
                query_one,
                query_two,
                key_one,
                key_two,
                value_proj,
                lambdas,
                norm_gain.reshape(1, head_v),
                out_proj,
            )
        )
    )


VMEM_LIMIT = 48 * 1024 * 1024


def solution(mesh):
    placed = (
        P("sp", None),
        P(None, "tp"),
        P(None, "tp"),
        P(None, "tp"),
        P(None, "tp"),
        P(None, "tp"),
        P("tp"),
        P(),
        P("tp", None),
    )

    def body(*args):
        groups = args[6].shape[0]
        split = groups * PLANE == mesh.shape["sp"] and mesh.shape["tp"] == 2
        return (fused_shards if split else shards)(*args)

    return jax.shard_map(
        body, mesh=mesh, in_specs=placed, out_specs=P("sp", None), check_vma=False
    )
```

```python
import math

import jax
import jax.numpy as jnp
from jax import lax
from jax.experimental import pallas as pl
from jax.experimental.pallas import tpu as pltpu
from jax.sharding import PartitionSpec as P

epsilon = 1e-06
masked_score = -1e30


def shards(
    hidden_in, query_one, query_two, key_one, key_two, value_proj, lambdas, norm_gain, out_proj
):
    heads_dev = lambdas.shape[0]
    head_qk = query_one.shape[1] // heads_dev
    head_v = value_proj.shape[1] // heads_dev
    width_q = heads_dev * head_qk
    score_scale = 1.75 * head_qk ** (-0.5)
    joined = jnp.concatenate((query_one, query_two, key_one, key_two, value_proj), axis=1)
    projected = jnp.dot(hidden_in, joined, preferred_element_type=jnp.float32).astype(jnp.bfloat16)
    tok_rows = projected.shape[0]
    key_values = projected[:, 2 * width_q :]
    my_index = lax.axis_index("sp")
    offset = my_index * tok_rows
    query_sets = (projected[:, : 2 * width_q],)
    position_sets = (offset + jnp.arange(tok_rows, dtype=jnp.int32),)
    groups = []
    for query_rows, positions in zip(query_sets, position_sets):
        group_rows = query_rows.shape[0]
        query_a = query_rows[:, :width_q].reshape(group_rows, heads_dev, head_qk)
        query_b = query_rows[:, width_q:].reshape(group_rows, heads_dev, head_qk)
        groups.append((query_a, query_b, positions, positions[group_rows - 1]))

    def one_map(queries, keys, value_rows, allowed, running_max, running_sum, accum):
        scores = (
            jnp.einsum("qhd,khd->hqk", queries, keys, preferred_element_type=jnp.float32)
            * score_scale
        )
        scores = jnp.where(allowed[None], scores, masked_score)
        new_max = jnp.maximum(running_max, jnp.max(scores, axis=-1))
        rescale = jnp.exp(running_max - new_max)
        weights = jnp.where(allowed[None], jnp.exp(scores - new_max[..., None]), 0.0)
        new_sum = running_sum * rescale + jnp.sum(weights, axis=-1)
        added = jnp.einsum(
            "hqk,khe->hqe",
            weights.astype(jnp.bfloat16),
            value_rows,
            preferred_element_type=jnp.float32,
        )
        return (new_max, new_sum, accum * rescale[..., None] + added)

    def absorb(group_state, group, kblock, kstart):
        query_a, query_b, positions, last_pos = group
        block_rows = kblock.shape[0]
        k_pos = kstart + jnp.arange(block_rows, dtype=jnp.int32)
        allowed = k_pos[None, :] <= positions[:, None]
        keys_a = kblock[:, :width_q].reshape(block_rows, heads_dev, head_qk)
        keys_b = kblock[:, width_q : 2 * width_q].reshape(block_rows, heads_dev, head_qk)
        value_rows = kblock[:, 2 * width_q :].reshape(block_rows, heads_dev, head_v)
        first_map = one_map(query_a, keys_a, value_rows, allowed, *group_state[:3])
        second_map = one_map(query_b, keys_b, value_rows, allowed, *group_state[3:])
        return first_map + second_map

    group = groups[0]
    group_rows = group[0].shape[0]
    start_max = jnp.full((heads_dev, group_rows), masked_score, jnp.float32)
    start_sum = jnp.zeros((heads_dev, group_rows), jnp.float32)
    start_acc = jnp.zeros((heads_dev, group_rows, head_v), jnp.float32)
    initial_list = [(start_max, start_sum, start_acc, start_max, start_sum, start_acc)]
    initial = tuple(initial_list)
    softmax_state = initial
    kv_piece = lax.all_gather(key_values, "sp", axis=0, tiled=True)
    piece_rows = kv_piece.shape[0]
    block_rows = math.gcd(piece_rows, 512)
    block_count = piece_rows // block_rows
    stacked = kv_piece.reshape(block_count, block_rows, kv_piece.shape[1])

    def absorb_step(carried, blocks_in):
        kblock, block_index = blocks_in
        kstart = block_index * block_rows
        renewed = []
        for group, group_state in zip(groups, carried):
            renewed.append(
                lax.cond(
                    kstart <= group[3],
                    lambda inner, group=group: absorb(inner, group, kblock, kstart),
                    lambda inner: inner,
                    group_state,
                )
            )
        return (tuple(renewed), None)

    softmax_state, _ = lax.scan(
        absorb_step, softmax_state, (stacked, jnp.arange(block_count, dtype=jnp.int32))
    )
    normed_sets = []
    for group_state in softmax_state:
        out_a = group_state[2] / group_state[1][..., None]
        out_b = group_state[5] / group_state[4][..., None]
        mixed_out = out_a - lambdas[:, None, None] * out_b
        scale_rows = lax.rsqrt(jnp.mean(mixed_out * mixed_out, axis=-1, keepdims=True) + epsilon)
        normed = (mixed_out * scale_rows * norm_gain).astype(jnp.bfloat16)
        group_rows = normed.shape[1]
        normed_sets.append(jnp.transpose(normed, (1, 0, 2)).reshape(group_rows, heads_dev * head_v))
    normed_all = normed_sets[0]
    partial_value = jnp.dot(normed_all, out_proj, preferred_element_type=jnp.float32)
    result = lax.psum(partial_value.astype(jnp.bfloat16), "tp")
    return result


MESH = pl.DeviceIdType.MESH
PLANE = 4
ROW_TILE = 256
OUT_TILE = 1024
LANES = 128


def fused_kernel(
    groups,
    score_scale,
    hidden_hbm,
    q1_hbm,
    q2_hbm,
    k1_hbm,
    k2_hbm,
    v_hbm,
    lam_hbm,
    gain_hbm,
    wo_hbm,
    out_ref,
    hid,
    wq1,
    wq2,
    wk1,
    wk2,
    wv,
    wo,
    lam_ref,
    gain_ref,
    k_out,
    v_out,
    q_out,
    k_all,
    v_all,
    q_all,
    n_out,
    n_all,
    max_all,
    sum_all,
    acc_all,
    load_sem,
    wo_send,
    wo_recv,
    zk_send,
    zk_recv,
    zv_send,
    zv_recv,
    q_send,
    q_recv,
    xk_send,
    xk_recv,
    xv_send,
    xv_recv,
    yk_send,
    yk_recv,
    yv_send,
    yv_recv,
    fk_send,
    fk_recv,
    fv_send,
    fv_recv,
    n_send,
    n_recv,
    r_send,
    r_recv,
):
    scope = jax.named_scope
    me = lax.axis_index("sp")
    core = lax.axis_index("tp")
    plane = me // PLANE
    spot = lax.rem(me, PLANE)
    x_spot = spot + 1 - 2 * lax.rem(spot, 2)
    y_spot = spot + 2 - 4 * (spot // 2)
    rows = hid.shape[0]
    qk = q1_hbm.shape[1] // groups
    width = 2 * qk
    head_v = v_hbm.shape[1] // groups

    def load(index, src, dst):
        return pltpu.make_async_copy(src, dst, load_sem.at[index])

    loads = [
        load(0, hidden_hbm, hid),
        load(1, k1_hbm, wk1),
        load(2, k2_hbm, wk2),
        load(3, v_hbm, wv),
        load(4, q1_hbm, wq1),
        load(5, q2_hbm, wq2),
        load(6, wo_hbm, wo.at[core]),
        load(7, lam_hbm, lam_ref),
        load(8, gain_hbm, gain_ref),
    ]
    for item in loads:
        item.start()
    barrier = pltpu.get_barrier_semaphore()

    def greet(index, tp_index):
        pl.semaphore_signal(barrier, inc=1, device_id=(index, tp_index), device_id_type=MESH)

    for step in range(1, groups):
        other = lax.rem(plane + step, groups) * PLANE + spot
        greet(other, core)
    greet(me, 1 - core)
    greet(plane * PLANE + x_spot, core)
    greet(plane * PLANE + y_spot, core)

    pending = []

    def send(src, dst, send_sem, recv_sem, index, tp_index):
        return pltpu.make_async_remote_copy(
            src_ref=src,
            dst_ref=dst,
            send_sem=send_sem,
            recv_sem=recv_sem,
            device_id=(index, tp_index),
            device_id_type=MESH,
        )

    def begin(*args):
        copy = send(*args)
        copy.start()
        pending.append(copy)

    def arrived(ref, recv_sem):
        pltpu.make_async_copy(ref, ref, recv_sem).wait()

    upper = plane >= groups // 2
    mirrored = jnp.where(upper, groups - 1 - plane, plane)

    def from_plane(step):
        if step == 0:
            return plane
        near = jnp.where(step - 1 < mirrored, step - 1, step)
        return jnp.where(upper, groups - 1 - near, near)

    def project(weight_ref):
        return jnp.dot(hid[...], weight_ref[...], preferred_element_type=jnp.float32)

    def joined(first, second, store):
        for head in range(groups):
            cut = slice(head * qk, (head + 1) * qk)
            store(head, jnp.concatenate((first[:, cut], second[:, cut]), axis=1))

    outer = jnp.logical_or(plane == 0, plane == groups - 1)
    inner = jnp.logical_not(outer)

    def z_copy(kind, step):
        target = from_plane(step)
        out, full, sems, recvs = {
            "k": (k_out, k_all.at[me], zk_send, zk_recv),
            "v": (v_out, v_all.at[me], zv_send, zv_recv),
            "q": (q_out, q_all.at[plane], q_send, q_recv),
        }[kind]
        return send(
            out.at[target],
            full,
            sems.at[step],
            recvs.at[plane],
            target * PLANE + spot,
            core,
        )

    def z_start(*items):
        for kind, step in items:
            z_copy(kind, step).start()

    def z_done(*items):
        for kind, step in items:
            z_copy(kind, step).wait_send()

    far = [step for step in range(2, groups)]

    def gate(index):
        with scope(f"gate#{index}"):

            @pl.when(outer)
            def _():
                z_done(("v", index))
                if index < groups - 1:
                    z_start(("k", index + 1), ("v", index + 1))
                else:
                    z_start(*(("q", step) for step in far))

            if index == groups - 1:

                @pl.when(inner)
                def _():
                    z_start(*(("q", step) for step in far))

    def x_block(step):
        return from_plane(step) * PLANE + x_spot

    def y_block(step):
        return from_plane(step) * PLANE + y_spot

    def spread_k(step):
        slot = k_all.at[from_plane(step) * PLANE + spot]
        begin(slot, slot, xk_send.at[step], xk_recv.at[step], plane * PLANE + x_spot, core)
        begin(slot, slot, yk_send.at[step], yk_recv.at[step], plane * PLANE + y_spot, core)

    def spread_v(step):
        slot = v_all.at[from_plane(step) * PLANE + spot]
        begin(slot, slot, yv_send.at[step], yv_recv.at[step], plane * PLANE + y_spot, core)
        begin(slot, slot, xv_send.at[step], xv_recv.at[step], plane * PLANE + x_spot, core)

    def forward(step):
        source = from_plane(step)
        with scope(f"zk#s={step}"):
            arrived(k_all.at[source * PLANE + spot], zk_recv.at[source])
        spread_k(step)
        with scope(f"zv#s={step}"):
            arrived(v_all.at[source * PLANE + spot], zv_recv.at[source])
        spread_v(step)

    def relay(step):
        with scope(f"rk#s={step}"):
            slot = k_all.at[x_block(step)]
            arrived(slot, xk_recv.at[step])
        begin(slot, slot, fk_send.at[step], fk_recv.at[step], plane * PLANE + y_spot, core)
        with scope(f"rv#s={step}"):
            slot = v_all.at[y_block(step)]
            arrived(slot, yv_recv.at[step])
        begin(slot, slot, fv_send.at[step], fv_recv.at[step], plane * PLANE + x_spot, core)

    def ready(step):
        far = from_plane(step) * PLANE + (PLANE - 1 - spot)
        with scope(f"ready#s={step}"):
            arrived(v_all.at[x_block(step)], xv_recv.at[step])
            arrived(k_all.at[y_block(step)], yk_recv.at[step])
            arrived(k_all.at[far], fk_recv.at[step])
            arrived(v_all.at[far], fv_recv.at[step])

    def ready_q(step):
        with scope(f"q#s={step}"):
            slot = q_all.at[from_plane(step)]
            arrived(slot, q_recv.at[from_plane(step)])

    with scope("w_hid"):
        loads[0].wait()
    with scope("w_k"):
        loads[1].wait()
        loads[2].wait()
    with scope("p_k"):
        first = project(wk1).astype(jnp.bfloat16)
        second = project(wk2).astype(jnp.bfloat16)

        def put_k(head, value):
            k_out[head] = value

        joined(first, second, put_k)
        k_all[me] = k_out[plane]
    with scope("barrier"):
        pl.semaphore_wait(barrier, groups - 1 + 3)
    z_start(("k", 1))
    pl.when(inner)(lambda: z_start(*(("k", step) for step in far)))
    spread_k(0)
    with scope("w_v"):
        loads[3].wait()
    with scope("p_v"):
        value = project(wv).astype(jnp.bfloat16)
        for head in range(groups):
            v_out[head] = value[:, head * head_v : (head + 1) * head_v]
        v_all[me] = v_out[plane]
    z_start(("v", 1))
    pl.when(inner)(lambda: z_start(*(("v", step) for step in far)))
    spread_v(0)
    with scope("w_q"):
        loads[4].wait()
        loads[5].wait()
    with scope("p_q"):
        first = (project(wq1) * score_scale).astype(jnp.bfloat16)
        second = (project(wq2) * score_scale).astype(jnp.bfloat16)

        def put_q(head, value):
            q_out[head] = value

        joined(first, second, put_q)
        q_all[plane] = q_out[plane]
    z_start(("q", 1))
    loads[6].wait()
    begin(wo.at[core], wo.at[core], wo_send, wo_recv, me, 1 - core)
    loads[7].wait()
    loads[8].wait()

    tile = ROW_TILE
    tiles = rows // tile
    chunk = PLANE * rows
    lane = lax.broadcasted_iota(jnp.int32, (tile, width), 1)

    def pair_tile(group, key_group, part, diagonal):
        begin_row = pl.multiple_of(part * tile, tile)
        queries = q_all[group, pl.ds(begin_row, tile), :]
        zero = jnp.zeros_like(queries)
        both = jnp.concatenate(
            (jnp.where(lane < qk, queries, zero), jnp.where(lane >= qk, queries, zero)), axis=0
        )
        keys = k_all[pl.ds(key_group * PLANE, PLANE)].reshape(chunk, width)
        values = v_all[pl.ds(key_group * PLANE, PLANE)].reshape(chunk, head_v)
        scores = lax.dot_general(
            both, keys, (((1,), (1,)), ((), ())), preferred_element_type=jnp.float32
        )
        cuts = [scores[:, c * LANES : (c + 1) * LANES] for c in range(chunk // LANES)]
        if diagonal:
            row = lax.rem(lax.broadcasted_iota(jnp.int32, (2 * tile, LANES), 0), tile)
            slack = (
                spot * rows
                + begin_row
                + row
                - lax.broadcasted_iota(jnp.int32, (2 * tile, LANES), 1)
            )
            cuts = [jnp.where(slack >= c * LANES, cut, masked_score) for c, cut in enumerate(cuts)]
        highest = cuts[0]
        for cut in cuts[1:]:
            highest = jnp.maximum(highest, cut)
        running_max = max_all[group, part]
        new_max = jnp.maximum(
            running_max,
            jnp.broadcast_to(jnp.max(highest, axis=-1, keepdims=True), highest.shape),
        )
        rescale = jnp.exp2(running_max - new_max)
        weights = [jnp.exp2(cut - new_max) for cut in cuts]
        new_sum = weights[0]
        for weight in weights[1:]:
            new_sum = new_sum + weight
        accum = jnp.dot(
            jnp.concatenate([weight.astype(jnp.bfloat16) for weight in weights], axis=1),
            values,
            preferred_element_type=jnp.float32,
        )
        max_all[group, part] = new_max
        sum_all[group, part] = sum_all[group, part] * rescale + new_sum
        acc_all[group, part] = acc_all[group, part] * rescale + accum

    def pair(group, key_group, diagonal):
        if not COMPUTE:
            return
        with scope("pair_d" if diagonal else "pair"):
            lax.fori_loop(
                0, tiles, lambda t, c: (pair_tile(group, key_group, t, diagonal), c)[1], 0
            )

    def meet(step, earlier):
        one, other = from_plane(step), from_plane(earlier)
        pair(jnp.maximum(one, other), jnp.minimum(one, other), False)

    def normed_copy(group):
        return send(
            n_out.at[group],
            n_all.at[core, plane],
            n_send.at[group],
            n_recv.at[plane],
            group * PLANE + spot,
            core,
        )

    def partner_copy(head):
        slot = n_all.at[core, head]
        return send(slot, slot, r_send.at[head], r_recv.at[head], me, 1 - core)

    lam = lam_ref[plane]
    gain = gain_ref[...]

    def finish(step):
        group = from_plane(step)
        if not COMPUTE:
            return

        def finish_tile(part, _):
            begin_row = pl.multiple_of(part * tile, tile)
            heads_out = acc_all[group, part] / jnp.sum(
                sum_all[group, part], axis=-1, keepdims=True
            )
            mixed = heads_out[:tile] - lam * heads_out[tile:]
            scale_rows = lax.rsqrt(jnp.mean(mixed * mixed, axis=-1, keepdims=True) + epsilon)
            normed = (mixed * scale_rows * gain).astype(jnp.bfloat16)
            n_out[group, pl.ds(begin_row, tile), :] = normed
            return 0

        lax.fori_loop(0, tiles, finish_tile, 0)

    def deliver(step):
        finish(step)
        group = from_plane(step)
        if step == 0:
            n_all[core, plane] = n_out[plane]
            partner_copy(plane).start()
        else:
            normed_copy(group).start()

    max_all[...] = jnp.full(max_all.shape, masked_score, jnp.float32)
    sum_all[...] = jnp.zeros(sum_all.shape, jnp.float32)
    acc_all[...] = jnp.zeros(acc_all.shape, jnp.float32)

    relay(0)
    gate(1)
    forward(1)
    ready(0)
    pair(plane, plane, True)
    forward(2)
    relay(1)
    gate(2)
    ready(1)
    ready_q(1)
    meet(1, 0)
    pair(from_plane(1), from_plane(1), True)
    relay(2)
    gate(3)
    forward(3)
    ready(2)
    ready_q(2)
    meet(2, 0)
    meet(2, 1)
    relay(3)
    pair(from_plane(2), from_plane(2), True)
    ready(3)
    ready_q(3)
    meet(3, 1)
    deliver(1)
    meet(3, 2)
    deliver(2)
    meet(3, 0)
    deliver(0)
    pair(from_plane(3), from_plane(3), True)
    deliver(3)

    for step in range(1, groups):
        head = from_plane(step)
        slot = n_all.at[core, head]
        with scope(f"n#s={step}"):
            arrived(slot, n_recv.at[head])
        partner_copy(head).start()

    def out_tiles(tp_index, first_part):
        normed = jnp.concatenate([n_all[tp_index, head] for head in range(groups)], axis=1)

        def out_tile(index, _):
            columns = pl.ds(pl.multiple_of(index * OUT_TILE, OUT_TILE), OUT_TILE)
            part = jnp.dot(normed, wo[tp_index, :, columns], preferred_element_type=jnp.float32)
            part = part.astype(jnp.bfloat16)
            if not first_part:
                part = (part.astype(jnp.float32) + out_ref[:, columns].astype(jnp.float32)).astype(
                    jnp.bfloat16
                )
            out_ref[:, columns] = part
            return 0

        lax.fori_loop(0, out_ref.shape[1] // OUT_TILE, out_tile, 0)

    with scope("out1"):
        out_tiles(core, True)
    with scope("rrecv"):
        arrived(wo.at[1 - core], wo_recv)
        for head in range(groups):
            arrived(n_all.at[1 - core, head], r_recv.at[head])
    with scope("out2"):
        out_tiles(1 - core, False)

    with scope("drain"):
        for copy in pending:
            copy.wait_send()
        pl.when(inner)(lambda: z_done(*(("v", step) for step in range(1, groups))))
        for step in range(1, groups):
            z_done(("k", step), ("q", step))
            normed_copy(from_plane(step)).wait_send()
        for head in range(groups):
            partner_copy(head).wait_send()


COMPUTE = True


def fused_shards(
    hidden_in, query_one, query_two, key_one, key_two, value_proj, lambdas, norm_gain, out_proj
):
    groups = lambdas.shape[0]
    rows, depth = hidden_in.shape
    head_qk = query_one.shape[1] // groups
    head_v = value_proj.shape[1] // groups
    width = 2 * head_qk
    blocks = groups * PLANE
    columns = out_proj.shape[1]
    score_scale = 1.75 * head_qk ** (-0.5) * math.log2(math.e)
    bf16 = jnp.bfloat16
    dma = pltpu.SemaphoreType.DMA
    hbm = pl.BlockSpec(memory_space=pltpu.HBM)
    vmem = pl.BlockSpec(memory_space=pltpu.VMEM)

    def body(*refs):
        fused_kernel(groups, score_scale, *refs)

    return pl.pallas_call(
        body,
        name="fused_attention",
        out_shape=jax.ShapeDtypeStruct((rows, columns), bf16),
        in_specs=[hbm] * 9,
        out_specs=vmem,
        scratch_shapes=[
            pltpu.VMEM(hidden_in.shape, bf16),
            pltpu.VMEM(query_one.shape, bf16),
            pltpu.VMEM(query_two.shape, bf16),
            pltpu.VMEM(key_one.shape, bf16),
            pltpu.VMEM(key_two.shape, bf16),
            pltpu.VMEM(value_proj.shape, bf16),
            pltpu.VMEM((2,) + out_proj.shape, bf16),
            pltpu.SMEM(lambdas.shape, jnp.float32),
            pltpu.VMEM((1, head_v), jnp.float32),
            pltpu.VMEM((groups, rows, width), bf16),
            pltpu.VMEM((groups, rows, head_v), bf16),
            pltpu.VMEM((groups, rows, width), bf16),
            pltpu.VMEM((blocks, rows, width), bf16),
            pltpu.VMEM((blocks, rows, head_v), bf16),
            pltpu.VMEM((groups, rows, width), bf16),
            pltpu.VMEM((groups, rows, head_v), bf16),
            pltpu.VMEM((2, groups, rows, head_v), bf16),
            pltpu.VMEM((groups, rows // ROW_TILE, 2 * ROW_TILE, LANES), jnp.float32),
            pltpu.VMEM((groups, rows // ROW_TILE, 2 * ROW_TILE, LANES), jnp.float32),
            pltpu.VMEM((groups, rows // ROW_TILE, 2 * ROW_TILE, head_v), jnp.float32),
            dma((9,)),
            dma,
            dma,
        ]
        + [dma((groups,))] * 22,
        compiler_params=pltpu.CompilerParams(
            collective_id=0, has_side_effects=True, vmem_limit_bytes=VMEM_LIMIT
        ),
    )(
        *(
            pltpu.with_memory_space_constraint(item, pltpu.HBM)
            for item in (
                hidden_in,
                query_one,
                query_two,
                key_one,
                key_two,
                value_proj,
                lambdas,
                norm_gain.reshape(1, head_v),
                out_proj,
            )
        )
    )


VMEM_LIMIT = 48 * 1024 * 1024


def solution(mesh):
    placed = (
        P("sp", None),
        P(None, "tp"),
        P(None, "tp"),
        P(None, "tp"),
        P(None, "tp"),
        P(None, "tp"),
        P("tp"),
        P(),
        P("tp", None),
    )

    def body(*args):
        groups = args[6].shape[0]
        split = groups * PLANE == mesh.shape["sp"] and mesh.shape["tp"] == 2
        return (fused_shards if split else shards)(*args)

    return jax.shard_map(
        body, mesh=mesh, in_specs=placed, out_specs=P("sp", None), check_vma=False
    )
```

```python
import math

import jax
import jax.numpy as jnp
from jax import lax
from jax.experimental import pallas as pl
from jax.experimental.pallas import tpu as pltpu
from jax.sharding import PartitionSpec as P

epsilon = 1e-06
masked_score = -1e30


def shards(
    hidden_in, query_one, query_two, key_one, key_two, value_proj, lambdas, norm_gain, out_proj
):
    heads_dev = lambdas.shape[0]
    head_qk = query_one.shape[1] // heads_dev
    head_v = value_proj.shape[1] // heads_dev
    width_q = heads_dev * head_qk
    score_scale = 1.75 * head_qk ** (-0.5)
    joined = jnp.concatenate((query_one, query_two, key_one, key_two, value_proj), axis=1)
    projected = jnp.dot(hidden_in, joined, preferred_element_type=jnp.float32).astype(jnp.bfloat16)
    tok_rows = projected.shape[0]
    key_values = projected[:, 2 * width_q :]
    my_index = lax.axis_index("sp")
    offset = my_index * tok_rows
    query_sets = (projected[:, : 2 * width_q],)
    position_sets = (offset + jnp.arange(tok_rows, dtype=jnp.int32),)
    groups = []
    for query_rows, positions in zip(query_sets, position_sets):
        group_rows = query_rows.shape[0]
        query_a = query_rows[:, :width_q].reshape(group_rows, heads_dev, head_qk)
        query_b = query_rows[:, width_q:].reshape(group_rows, heads_dev, head_qk)
        groups.append((query_a, query_b, positions, positions[group_rows - 1]))

    def one_map(queries, keys, value_rows, allowed, running_max, running_sum, accum):
        scores = (
            jnp.einsum("qhd,khd->hqk", queries, keys, preferred_element_type=jnp.float32)
            * score_scale
        )
        scores = jnp.where(allowed[None], scores, masked_score)
        new_max = jnp.maximum(running_max, jnp.max(scores, axis=-1))
        rescale = jnp.exp(running_max - new_max)
        weights = jnp.where(allowed[None], jnp.exp(scores - new_max[..., None]), 0.0)
        new_sum = running_sum * rescale + jnp.sum(weights, axis=-1)
        added = jnp.einsum(
            "hqk,khe->hqe",
            weights.astype(jnp.bfloat16),
            value_rows,
            preferred_element_type=jnp.float32,
        )
        return (new_max, new_sum, accum * rescale[..., None] + added)

    def absorb(group_state, group, kblock, kstart):
        query_a, query_b, positions, last_pos = group
        block_rows = kblock.shape[0]
        k_pos = kstart + jnp.arange(block_rows, dtype=jnp.int32)
        allowed = k_pos[None, :] <= positions[:, None]
        keys_a = kblock[:, :width_q].reshape(block_rows, heads_dev, head_qk)
        keys_b = kblock[:, width_q : 2 * width_q].reshape(block_rows, heads_dev, head_qk)
        value_rows = kblock[:, 2 * width_q :].reshape(block_rows, heads_dev, head_v)
        first_map = one_map(query_a, keys_a, value_rows, allowed, *group_state[:3])
        second_map = one_map(query_b, keys_b, value_rows, allowed, *group_state[3:])
        return first_map + second_map

    group = groups[0]
    group_rows = group[0].shape[0]
    start_max = jnp.full((heads_dev, group_rows), masked_score, jnp.float32)
    start_sum = jnp.zeros((heads_dev, group_rows), jnp.float32)
    start_acc = jnp.zeros((heads_dev, group_rows, head_v), jnp.float32)
    initial_list = [(start_max, start_sum, start_acc, start_max, start_sum, start_acc)]
    initial = tuple(initial_list)
    softmax_state = initial
    kv_piece = lax.all_gather(key_values, "sp", axis=0, tiled=True)
    piece_rows = kv_piece.shape[0]
    block_rows = math.gcd(piece_rows, 512)
    block_count = piece_rows // block_rows
    stacked = kv_piece.reshape(block_count, block_rows, kv_piece.shape[1])

    def absorb_step(carried, blocks_in):
        kblock, block_index = blocks_in
        kstart = block_index * block_rows
        renewed = []
        for group, group_state in zip(groups, carried):
            renewed.append(
                lax.cond(
                    kstart <= group[3],
                    lambda inner, group=group: absorb(inner, group, kblock, kstart),
                    lambda inner: inner,
                    group_state,
                )
            )
        return (tuple(renewed), None)

    softmax_state, _ = lax.scan(
        absorb_step, softmax_state, (stacked, jnp.arange(block_count, dtype=jnp.int32))
    )
    normed_sets = []
    for group_state in softmax_state:
        out_a = group_state[2] / group_state[1][..., None]
        out_b = group_state[5] / group_state[4][..., None]
        mixed_out = out_a - lambdas[:, None, None] * out_b
        scale_rows = lax.rsqrt(jnp.mean(mixed_out * mixed_out, axis=-1, keepdims=True) + epsilon)
        normed = (mixed_out * scale_rows * norm_gain).astype(jnp.bfloat16)
        group_rows = normed.shape[1]
        normed_sets.append(jnp.transpose(normed, (1, 0, 2)).reshape(group_rows, heads_dev * head_v))
    normed_all = normed_sets[0]
    partial_value = jnp.dot(normed_all, out_proj, preferred_element_type=jnp.float32)
    result = lax.psum(partial_value.astype(jnp.bfloat16), "tp")
    return result


MESH = pl.DeviceIdType.MESH
PLANE = 4
ROW_TILE = 256
OUT_TILE = 1024
LANES = 128


def fused_kernel(
    groups,
    score_scale,
    hidden_hbm,
    q1_hbm,
    q2_hbm,
    k1_hbm,
    k2_hbm,
    v_hbm,
    lam_hbm,
    gain_hbm,
    wo_hbm,
    out_ref,
    hid,
    wq1,
    wq2,
    wk1,
    wk2,
    wv,
    wo,
    lam_ref,
    gain_ref,
    k_out,
    v_out,
    q_out,
    k_all,
    v_all,
    q_all,
    n_out,
    n_all,
    max_all,
    sum_all,
    acc_all,
    load_sem,
    wo_send,
    wo_recv,
    zk_send,
    zk_recv,
    zv_send,
    zv_recv,
    q_send,
    q_recv,
    xk_send,
    xk_recv,
    xv_send,
    xv_recv,
    yk_send,
    yk_recv,
    yv_send,
    yv_recv,
    fk_send,
    fk_recv,
    fv_send,
    fv_recv,
    n_send,
    n_recv,
    r_send,
    r_recv,
):
    scope = jax.named_scope
    me = lax.axis_index("sp")
    core = lax.axis_index("tp")
    plane = me // PLANE
    spot = lax.rem(me, PLANE)
    x_spot = spot + 1 - 2 * lax.rem(spot, 2)
    y_spot = spot + 2 - 4 * (spot // 2)
    rows = hid.shape[0]
    qk = q1_hbm.shape[1] // groups
    width = 2 * qk
    head_v = v_hbm.shape[1] // groups

    def load(index, src, dst):
        return pltpu.make_async_copy(src, dst, load_sem.at[index])

    loads = [
        load(0, hidden_hbm, hid),
        load(1, k1_hbm, wk1),
        load(2, k2_hbm, wk2),
        load(3, v_hbm, wv),
        load(4, q1_hbm, wq1),
        load(5, q2_hbm, wq2),
        load(6, wo_hbm, wo.at[core]),
        load(7, lam_hbm, lam_ref),
        load(8, gain_hbm, gain_ref),
    ]
    for item in loads:
        item.start()
    barrier = pltpu.get_barrier_semaphore()

    def greet(index, tp_index):
        pl.semaphore_signal(barrier, inc=1, device_id=(index, tp_index), device_id_type=MESH)

    for step in range(1, groups):
        other = lax.rem(plane + step, groups) * PLANE + spot
        greet(other, core)
    greet(me, 1 - core)
    greet(plane * PLANE + x_spot, core)
    greet(plane * PLANE + y_spot, core)

    pending = []

    def send(src, dst, send_sem, recv_sem, index, tp_index):
        return pltpu.make_async_remote_copy(
            src_ref=src,
            dst_ref=dst,
            send_sem=send_sem,
            recv_sem=recv_sem,
            device_id=(index, tp_index),
            device_id_type=MESH,
        )

    def begin(*args):
        copy = send(*args)
        copy.start()
        pending.append(copy)

    def arrived(ref, recv_sem):
        pltpu.make_async_copy(ref, ref, recv_sem).wait()

    half = groups // 2
    upper = plane >= half
    lower = jnp.logical_not(upper)
    base = jnp.where(upper, half, 0)
    def from_plane(step):
        if step < half:
            return base + lax.rem(plane + step, half)
        return (half - base) + (step - half)

    def project(weight_ref):
        return jnp.dot(hid[...], weight_ref[...], preferred_element_type=jnp.float32)

    def joined(first, second, store):
        for head in range(groups):
            cut = slice(head * qk, (head + 1) * qk)
            store(head, jnp.concatenate((first[:, cut], second[:, cut]), axis=1))

    def z_copy(kind, step):
        target = from_plane(step)
        out, full, sems, recvs = {
            "k": (k_out, k_all.at[me], zk_send, zk_recv),
            "v": (v_out, v_all.at[me], zv_send, zv_recv),
            "q": (q_out, q_all.at[plane], q_send, q_recv),
        }[kind]
        return send(
            out.at[target],
            full,
            sems.at[step],
            recvs.at[plane],
            target * PLANE + spot,
            core,
        )

    def z_start(*items):
        for kind, step in items:
            z_copy(kind, step).start()

    def z_done(*items):
        for kind, step in items:
            z_copy(kind, step).wait_send()

    def launch(moment):
        for index in range(groups):
            items = SENDS[index].get(moment, "").split()
            if items:

                @pl.when(plane == index)
                def _():
                    z_start(*((item[0], int(item[1])) for item in items))

    def x_block(step):
        return from_plane(step) * PLANE + x_spot

    def y_block(step):
        return from_plane(step) * PLANE + y_spot

    def spread_k(step):
        slot = k_all.at[from_plane(step) * PLANE + spot]
        begin(slot, slot, xk_send.at[step], xk_recv.at[step], plane * PLANE + x_spot, core)
        begin(slot, slot, yk_send.at[step], yk_recv.at[step], plane * PLANE + y_spot, core)

    def spread_v(step):
        slot = v_all.at[from_plane(step) * PLANE + spot]
        begin(slot, slot, yv_send.at[step], yv_recv.at[step], plane * PLANE + y_spot, core)
        begin(slot, slot, xv_send.at[step], xv_recv.at[step], plane * PLANE + x_spot, core)

    def forward(step):
        source = from_plane(step)
        with scope(f"zk#s={step}"):
            arrived(k_all.at[source * PLANE + spot], zk_recv.at[source])
        spread_k(step)
        with scope(f"zv#s={step}"):
            arrived(v_all.at[source * PLANE + spot], zv_recv.at[source])
        spread_v(step)

    def relay(step):
        with scope(f"rk#s={step}"):
            slot = k_all.at[x_block(step)]
            arrived(slot, xk_recv.at[step])
        begin(slot, slot, fk_send.at[step], fk_recv.at[step], plane * PLANE + y_spot, core)
        with scope(f"rv#s={step}"):
            slot = v_all.at[y_block(step)]
            arrived(slot, yv_recv.at[step])
        begin(slot, slot, fv_send.at[step], fv_recv.at[step], plane * PLANE + x_spot, core)

    def ready(step):
        far = from_plane(step) * PLANE + (PLANE - 1 - spot)
        with scope(f"ready#s={step}"):
            arrived(v_all.at[x_block(step)], xv_recv.at[step])
            arrived(k_all.at[y_block(step)], yk_recv.at[step])
            arrived(k_all.at[far], fk_recv.at[step])
            arrived(v_all.at[far], fv_recv.at[step])

    def ready_q(step):
        with scope(f"q#s={step}"):
            slot = q_all.at[from_plane(step)]
            arrived(slot, q_recv.at[from_plane(step)])

    with scope("w_hid"):
        loads[0].wait()
    with scope("w_k"):
        loads[1].wait()
        loads[2].wait()
    with scope("p_k"):
        first = project(wk1).astype(jnp.bfloat16)
        second = project(wk2).astype(jnp.bfloat16)

        def put_k(head, value):
            k_out[head] = value

        joined(first, second, put_k)
        k_all[me] = k_out[plane]
    with scope("barrier"):
        pl.semaphore_wait(barrier, groups - 1 + 3)
    launch("k")
    spread_k(0)
    with scope("w_v"):
        loads[3].wait()
    with scope("p_v"):
        value = project(wv).astype(jnp.bfloat16)
        for head in range(groups):
            v_out[head] = value[:, head * head_v : (head + 1) * head_v]
        v_all[me] = v_out[plane]
    launch("v")
    spread_v(0)
    with scope("w_q"):
        loads[4].wait()
        loads[5].wait()
    with scope("p_q"):
        first = (project(wq1) * score_scale).astype(jnp.bfloat16)
        second = (project(wq2) * score_scale).astype(jnp.bfloat16)

        def put_q(head, value):
            q_out[head] = value

        joined(first, second, put_q)
        q_all[plane] = q_out[plane]
    launch("q")
    loads[6].wait()
    begin(wo.at[core], wo.at[core], wo_send, wo_recv, me, 1 - core)
    loads[7].wait()
    loads[8].wait()

    tile = ROW_TILE
    tiles = rows // tile
    chunk = PLANE * rows
    lane = lax.broadcasted_iota(jnp.int32, (tile, width), 1)

    def pair_tile(group, key_group, part, diagonal):
        begin_row = pl.multiple_of(part * tile, tile)
        queries = q_all[group, pl.ds(begin_row, tile), :]
        zero = jnp.zeros_like(queries)
        both = jnp.concatenate(
            (jnp.where(lane < qk, queries, zero), jnp.where(lane >= qk, queries, zero)), axis=0
        )
        keys = k_all[pl.ds(key_group * PLANE, PLANE)].reshape(chunk, width)
        values = v_all[pl.ds(key_group * PLANE, PLANE)].reshape(chunk, head_v)
        scores = lax.dot_general(
            both, keys, (((1,), (1,)), ((), ())), preferred_element_type=jnp.float32
        )
        cuts = [scores[:, c * LANES : (c + 1) * LANES] for c in range(chunk // LANES)]
        if diagonal:
            row = lax.rem(lax.broadcasted_iota(jnp.int32, (2 * tile, LANES), 0), tile)
            slack = (
                spot * rows
                + begin_row
                + row
                - lax.broadcasted_iota(jnp.int32, (2 * tile, LANES), 1)
            )
            cuts = [jnp.where(slack >= c * LANES, cut, masked_score) for c, cut in enumerate(cuts)]
        highest = cuts[0]
        for cut in cuts[1:]:
            highest = jnp.maximum(highest, cut)
        running_max = max_all[group, part]
        new_max = jnp.maximum(
            running_max,
            jnp.broadcast_to(jnp.max(highest, axis=-1, keepdims=True), highest.shape),
        )
        rescale = jnp.exp2(running_max - new_max)
        weights = [jnp.exp2(cut - new_max) for cut in cuts]
        new_sum = weights[0]
        for weight in weights[1:]:
            new_sum = new_sum + weight
        accum = jnp.dot(
            jnp.concatenate([weight.astype(jnp.bfloat16) for weight in weights], axis=1),
            values,
            preferred_element_type=jnp.float32,
        )
        max_all[group, part] = new_max
        sum_all[group, part] = sum_all[group, part] * rescale + new_sum
        acc_all[group, part] = acc_all[group, part] * rescale + accum

    def pair(group, key_group, diagonal):
        if not COMPUTE:
            return
        with scope("pair_d" if diagonal else "pair"):
            lax.fori_loop(
                0, tiles, lambda t, c: (pair_tile(group, key_group, t, diagonal), c)[1], 0
            )

    def meet(step, earlier):
        one, other = from_plane(step), from_plane(earlier)
        pair(jnp.maximum(one, other), jnp.minimum(one, other), False)

    def normed_copy(group):
        return send(
            n_out.at[group],
            n_all.at[core, plane],
            n_send.at[group],
            n_recv.at[plane],
            group * PLANE + spot,
            core,
        )

    def partner_copy(head):
        slot = n_all.at[core, head]
        return send(slot, slot, r_send.at[head], r_recv.at[head], me, 1 - core)

    lam = lam_ref[plane]
    gain = gain_ref[...]

    def finish(step):
        group = from_plane(step)
        if not COMPUTE:
            return

        def finish_tile(part, _):
            begin_row = pl.multiple_of(part * tile, tile)
            heads_out = acc_all[group, part] / jnp.sum(
                sum_all[group, part], axis=-1, keepdims=True
            )
            mixed = heads_out[:tile] - lam * heads_out[tile:]
            scale_rows = lax.rsqrt(jnp.mean(mixed * mixed, axis=-1, keepdims=True) + epsilon)
            normed = (mixed * scale_rows * gain).astype(jnp.bfloat16)
            n_out[group, pl.ds(begin_row, tile), :] = normed
            return 0

        lax.fori_loop(0, tiles, finish_tile, 0)

    def deliver(step):
        finish(step)
        group = from_plane(step)
        if step == 0:
            n_all[core, plane] = n_out[plane]
            partner_copy(plane).start()
        else:
            normed_copy(group).start()

    max_all[...] = jnp.full(max_all.shape, masked_score, jnp.float32)
    sum_all[...] = jnp.zeros(sum_all.shape, jnp.float32)
    acc_all[...] = jnp.zeros(acc_all.shape, jnp.float32)

    def diagonal(step):
        pair(from_plane(step), from_plane(step), True)

    relay(0)
    forward(1)
    launch("c")
    ready(0)
    launch("d")
    diagonal(0)
    forward(2)
    relay(1)
    launch("e")
    ready(1)
    launch("f")
    ready_q(1)
    meet(1, 0)
    diagonal(1)

    relay(2)
    forward(3)

    @pl.when(lower)
    def _():
        deliver(1)
        deliver(0)

    ready(2)
    ready_q(2)
    meet(2, 0)
    meet(2, 1)
    diagonal(2)
    deliver(2)
    relay(3)
    ready_q(3)
    meet(3, 2)

    @pl.when(lower)
    def _():
        meet(3, 0)
        meet(3, 1)

    ready(3)
    diagonal(3)
    deliver(3)

    @pl.when(upper)
    def _():
        meet(3, 1)
        deliver(1)
        meet(3, 0)
        deliver(0)

    for step in range(1, groups):
        head = from_plane(step)
        slot = n_all.at[core, head]
        with scope(f"n#s={step}"):
            arrived(slot, n_recv.at[head])
        partner_copy(head).start()

    def out_tiles(tp_index, first_part):
        normed = jnp.concatenate([n_all[tp_index, head] for head in range(groups)], axis=1)

        def out_tile(index, _):
            columns = pl.ds(pl.multiple_of(index * OUT_TILE, OUT_TILE), OUT_TILE)
            part = jnp.dot(normed, wo[tp_index, :, columns], preferred_element_type=jnp.float32)
            part = part.astype(jnp.bfloat16)
            if not first_part:
                part = (part.astype(jnp.float32) + out_ref[:, columns].astype(jnp.float32)).astype(
                    jnp.bfloat16
                )
            out_ref[:, columns] = part
            return 0

        lax.fori_loop(0, out_ref.shape[1] // OUT_TILE, out_tile, 0)

    with scope("out1"):
        out_tiles(core, True)
    with scope("rrecv"):
        arrived(wo.at[1 - core], wo_recv)
        for head in range(groups):
            arrived(n_all.at[1 - core, head], r_recv.at[head])
    with scope("out2"):
        out_tiles(1 - core, False)

    with scope("drain"):
        for copy in pending:
            copy.wait_send()
        for step in range(1, groups):
            z_done(("k", step), ("v", step), ("q", step))
            normed_copy(from_plane(step)).wait_send()
        for head in range(groups):
            partner_copy(head).wait_send()


COMPUTE = True
SENDS = (
    {"k": "k1", "v": "v1 k3 v3 k2 v2", "q": "q1", "f": "q2 q3"},
    {"k": "k1 k2", "v": "v1 v2 k3 v3", "q": "q1 q2 q3"},
    {"k": "k1 k3", "v": "v1 v3 k2 v2", "q": "q1 q3 q2"},
    {"k": "k1", "v": "v1", "q": "q1", "d": "k3 v3 k2 v2 q3 q2"},
)


def fused_shards(
    hidden_in, query_one, query_two, key_one, key_two, value_proj, lambdas, norm_gain, out_proj
):
    groups = lambdas.shape[0]
    rows, depth = hidden_in.shape
    head_qk = query_one.shape[1] // groups
    head_v = value_proj.shape[1] // groups
    width = 2 * head_qk
    blocks = groups * PLANE
    columns = out_proj.shape[1]
    score_scale = 1.75 * head_qk ** (-0.5) * math.log2(math.e)
    bf16 = jnp.bfloat16
    dma = pltpu.SemaphoreType.DMA
    hbm = pl.BlockSpec(memory_space=pltpu.HBM)
    vmem = pl.BlockSpec(memory_space=pltpu.VMEM)

    def body(*refs):
        fused_kernel(groups, score_scale, *refs)

    return pl.pallas_call(
        body,
        name="fused_attention",
        out_shape=jax.ShapeDtypeStruct((rows, columns), bf16),
        in_specs=[hbm] * 9,
        out_specs=vmem,
        scratch_shapes=[
            pltpu.VMEM(hidden_in.shape, bf16),
            pltpu.VMEM(query_one.shape, bf16),
            pltpu.VMEM(query_two.shape, bf16),
            pltpu.VMEM(key_one.shape, bf16),
            pltpu.VMEM(key_two.shape, bf16),
            pltpu.VMEM(value_proj.shape, bf16),
            pltpu.VMEM((2,) + out_proj.shape, bf16),
            pltpu.SMEM(lambdas.shape, jnp.float32),
            pltpu.VMEM((1, head_v), jnp.float32),
            pltpu.VMEM((groups, rows, width), bf16),
            pltpu.VMEM((groups, rows, head_v), bf16),
            pltpu.VMEM((groups, rows, width), bf16),
            pltpu.VMEM((blocks, rows, width), bf16),
            pltpu.VMEM((blocks, rows, head_v), bf16),
            pltpu.VMEM((groups, rows, width), bf16),
            pltpu.VMEM((groups, rows, head_v), bf16),
            pltpu.VMEM((2, groups, rows, head_v), bf16),
            pltpu.VMEM((groups, rows // ROW_TILE, 2 * ROW_TILE, LANES), jnp.float32),
            pltpu.VMEM((groups, rows // ROW_TILE, 2 * ROW_TILE, LANES), jnp.float32),
            pltpu.VMEM((groups, rows // ROW_TILE, 2 * ROW_TILE, head_v), jnp.float32),
            dma((9,)),
            dma,
            dma,
        ]
        + [dma((groups,))] * 22,
        compiler_params=pltpu.CompilerParams(
            collective_id=0, has_side_effects=True, vmem_limit_bytes=VMEM_LIMIT
        ),
    )(
        *(
            pltpu.with_memory_space_constraint(item, pltpu.HBM)
            for item in (
                hidden_in,
                query_one,
                query_two,
                key_one,
                key_two,
                value_proj,
                lambdas,
                norm_gain.reshape(1, head_v),
                out_proj,
            )
        )
    )


VMEM_LIMIT = 48 * 1024 * 1024


def solution(mesh):
    placed = (
        P("sp", None),
        P(None, "tp"),
        P(None, "tp"),
        P(None, "tp"),
        P(None, "tp"),
        P(None, "tp"),
        P("tp"),
        P(),
        P("tp", None),
    )

    def body(*args):
        groups = args[6].shape[0]
        split = groups * PLANE == mesh.shape["sp"] and mesh.shape["tp"] == 2
        return (fused_shards if split else shards)(*args)

    return jax.shard_map(
        body, mesh=mesh, in_specs=placed, out_specs=P("sp", None), check_vma=False
    )
```

```python
import functools
import math

import jax
import jax.numpy as jnp
from jax import lax
from jax.experimental import pallas as pl
from jax.experimental.pallas import tpu as pltpu
from jax.sharding import PartitionSpec as P

epsilon = 1e-06
masked_score = -1e30


def shards(
    hidden_in, query_one, query_two, key_one, key_two, value_proj, lambdas, norm_gain, out_proj
):
    heads_dev = lambdas.shape[0]
    head_qk = query_one.shape[1] // heads_dev
    head_v = value_proj.shape[1] // heads_dev
    width_q = heads_dev * head_qk
    score_scale = 1.75 * head_qk ** (-0.5)
    joined = jnp.concatenate((query_one, query_two, key_one, key_two, value_proj), axis=1)
    projected = jnp.dot(hidden_in, joined, preferred_element_type=jnp.float32).astype(jnp.bfloat16)
    tok_rows = projected.shape[0]
    key_values = projected[:, 2 * width_q :]
    my_index = lax.axis_index("sp")
    offset = my_index * tok_rows
    query_sets = (projected[:, : 2 * width_q],)
    position_sets = (offset + jnp.arange(tok_rows, dtype=jnp.int32),)
    groups = []
    for query_rows, positions in zip(query_sets, position_sets):
        group_rows = query_rows.shape[0]
        query_a = query_rows[:, :width_q].reshape(group_rows, heads_dev, head_qk)
        query_b = query_rows[:, width_q:].reshape(group_rows, heads_dev, head_qk)
        groups.append((query_a, query_b, positions, positions[group_rows - 1]))

    def one_map(queries, keys, value_rows, allowed, running_max, running_sum, accum):
        scores = (
            jnp.einsum("qhd,khd->hqk", queries, keys, preferred_element_type=jnp.float32)
            * score_scale
        )
        scores = jnp.where(allowed[None], scores, masked_score)
        new_max = jnp.maximum(running_max, jnp.max(scores, axis=-1))
        rescale = jnp.exp(running_max - new_max)
        weights = jnp.where(allowed[None], jnp.exp(scores - new_max[..., None]), 0.0)
        new_sum = running_sum * rescale + jnp.sum(weights, axis=-1)
        added = jnp.einsum(
            "hqk,khe->hqe",
            weights.astype(jnp.bfloat16),
            value_rows,
            preferred_element_type=jnp.float32,
        )
        return (new_max, new_sum, accum * rescale[..., None] + added)

    def absorb(group_state, group, kblock, kstart):
        query_a, query_b, positions, last_pos = group
        block_rows = kblock.shape[0]
        k_pos = kstart + jnp.arange(block_rows, dtype=jnp.int32)
        allowed = k_pos[None, :] <= positions[:, None]
        keys_a = kblock[:, :width_q].reshape(block_rows, heads_dev, head_qk)
        keys_b = kblock[:, width_q : 2 * width_q].reshape(block_rows, heads_dev, head_qk)
        value_rows = kblock[:, 2 * width_q :].reshape(block_rows, heads_dev, head_v)
        first_map = one_map(query_a, keys_a, value_rows, allowed, *group_state[:3])
        second_map = one_map(query_b, keys_b, value_rows, allowed, *group_state[3:])
        return first_map + second_map

    group = groups[0]
    group_rows = group[0].shape[0]
    start_max = jnp.full((heads_dev, group_rows), masked_score, jnp.float32)
    start_sum = jnp.zeros((heads_dev, group_rows), jnp.float32)
    start_acc = jnp.zeros((heads_dev, group_rows, head_v), jnp.float32)
    initial_list = [(start_max, start_sum, start_acc, start_max, start_sum, start_acc)]
    initial = tuple(initial_list)
    softmax_state = initial
    kv_piece = lax.all_gather(key_values, "sp", axis=0, tiled=True)
    piece_rows = kv_piece.shape[0]
    block_rows = math.gcd(piece_rows, 512)
    block_count = piece_rows // block_rows
    stacked = kv_piece.reshape(block_count, block_rows, kv_piece.shape[1])

    def absorb_step(carried, blocks_in):
        kblock, block_index = blocks_in
        kstart = block_index * block_rows
        renewed = []
        for group, group_state in zip(groups, carried):
            renewed.append(
                lax.cond(
                    kstart <= group[3],
                    lambda inner, group=group: absorb(inner, group, kblock, kstart),
                    lambda inner: inner,
                    group_state,
                )
            )
        return (tuple(renewed), None)

    softmax_state, _ = lax.scan(
        absorb_step, softmax_state, (stacked, jnp.arange(block_count, dtype=jnp.int32))
    )
    normed_sets = []
    for group_state in softmax_state:
        out_a = group_state[2] / group_state[1][..., None]
        out_b = group_state[5] / group_state[4][..., None]
        mixed_out = out_a - lambdas[:, None, None] * out_b
        scale_rows = lax.rsqrt(jnp.mean(mixed_out * mixed_out, axis=-1, keepdims=True) + epsilon)
        normed = (mixed_out * scale_rows * norm_gain).astype(jnp.bfloat16)
        group_rows = normed.shape[1]
        normed_sets.append(jnp.transpose(normed, (1, 0, 2)).reshape(group_rows, heads_dev * head_v))
    normed_all = normed_sets[0]
    partial_value = jnp.dot(normed_all, out_proj, preferred_element_type=jnp.float32)
    result = lax.psum(partial_value.astype(jnp.bfloat16), "tp")
    return result


MESH = pl.DeviceIdType.MESH
PLANE = 4
ROW_TILE = 256
OUT_TILE = 2048
LANES = 128


def fused_kernel(
    groups,
    score_scale,
    hidden_hbm,
    q1_hbm,
    q2_hbm,
    k1_hbm,
    k2_hbm,
    v_hbm,
    lam_hbm,
    gain_hbm,
    wo_hbm,
    out_ref,
    hid,
    wq1,
    wq2,
    wk1,
    wk2,
    wv,
    wo,
    lam_ref,
    lam_all,
    gain_ref,
    k_out,
    v_out,
    q_out,
    k_all,
    v_all,
    q_all,
    n_out,
    n_all,
    max_all,
    sum_all,
    acc_all,
    out_acc,
    load_sem,
    wo_send,
    wo_recv,
    lam_send,
    lam_recv,
    zk_send,
    zk_recv,
    zv_send,
    zv_recv,
    q_send,
    q_recv,
    xk_send,
    xk_recv,
    xv_send,
    xv_recv,
    yk_send,
    yk_recv,
    yv_send,
    yv_recv,
    fk_send,
    fk_recv,
    fv_send,
    fv_recv,
    n_send,
    n_recv,
    r_send,
    r_recv,
):
    scope = jax.named_scope
    me = lax.axis_index("sp")
    core = lax.axis_index("tp")
    plane = me // PLANE
    spot = lax.rem(me, PLANE)
    x = lax.rem(spot, 2)
    y = spot // 2
    mine = 2 * core + x
    home = core == y
    away = core != y
    rows = hid.shape[0]
    qk = q1_hbm.shape[1] // groups
    width = 2 * qk
    head_v = v_hbm.shape[1] // groups

    def load(index, src, dst):
        return pltpu.make_async_copy(src, dst, load_sem.at[index])

    loads = [
        load(0, hidden_hbm, hid),
        load(1, k1_hbm, wk1),
        load(2, k2_hbm, wk2),
        load(3, v_hbm, wv),
        load(4, q1_hbm, wq1),
        load(5, q2_hbm, wq2),
        load(6, wo_hbm, wo.at[core]),
        load(7, lam_hbm, lam_ref),
        load(8, gain_hbm, gain_ref),
    ]
    for item in loads:
        item.start()
    barrier = pltpu.get_barrier_semaphore()

    def greet(index, tp_index):
        pl.semaphore_signal(barrier, inc=1, device_id=(index, tp_index), device_id_type=MESH)

    def owner(index):
        return index * PLANE + mine, y

    for step in range(1, groups):
        greet(*owner(lax.rem(plane + step, groups)))
    pl.when(away)(lambda: greet(*owner(plane)))
    greet(me, 1 - core)
    greet(me + 1 - 2 * x, core)

    def send(src, dst, send_sem, recv_sem, index, tp_index):
        return pltpu.make_async_remote_copy(
            src_ref=src,
            dst_ref=dst,
            send_sem=send_sem,
            recv_sem=recv_sem,
            device_id=(index, tp_index),
            device_id_type=MESH,
        )

    def arrived(ref, recv_sem):
        pltpu.make_async_copy(ref, ref, recv_sem).wait()

    half = groups // 2
    upper = plane >= half
    lower = jnp.logical_not(upper)
    base = jnp.where(upper, half, 0)
    swapped = lax.rem(plane, half) == 0

    def from_plane(step):
        if step < half:
            return base + lax.rem(plane + step, half)
        return (half - base) + jnp.where(swapped, groups - 1 - step, step - half)

    def project(weight_ref):
        return jnp.dot(hid[...], weight_ref[...], preferred_element_type=jnp.float32)

    def joined(first, second, store):
        for head in range(groups):
            cut = slice(head * qk, (head + 1) * qk)
            store(head, jnp.concatenate((first[:, cut], second[:, cut]), axis=1))

    def z_copy(kind, step):
        target = from_plane(step)
        out, full, sems, recvs = {
            "k": (k_out, k_all.at[me], zk_send, zk_recv),
            "v": (v_out, v_all.at[me], zv_send, zv_recv),
            "q": (q_out, q_all.at[plane], q_send, q_recv),
        }[kind]
        return send(
            out.at[target],
            full,
            sems.at[step],
            recvs.at[plane],
            *owner(target),
        )

    def z_start(*items):
        for kind, step in items:
            z_copy(kind, step).start()

    def z_done(*items):
        for kind, step in items:
            z_copy(kind, step).wait_send()

    def perform(items):
        for item in items:
            kind, step = item[0], int(item[1])
            if kind in "kvq":
                z_copy(kind, step).start()
            else:
                {"z": forward, "r": relay, "w": ready, "a": ready_q}[kind](step)

    places = [
        jnp.logical_and(plane == index, place) for index in range(groups) for place in (home, away)
    ]

    def moment(name):
        texts = [order.get(name, "") for order in ORDER]
        lists = [[text[i : i + 2] for i in range(0, len(text), 2)] for text in texts]
        if all(items == lists[0] for items in lists):
            perform(lists[0])
            return
        for items in dict.fromkeys(map(tuple, lists)):
            if items:
                place = functools.reduce(
                    jnp.logical_or, [p for p, other in zip(places, lists) if tuple(other) == items]
                )
                pl.when(place)(lambda items=items: perform(items))

    def x_block(step):
        return from_plane(step) * PLANE + mine + 1 - 2 * x

    def y_block(step):
        return from_plane(step) * PLANE + mine + 2 - 4 * core

    def to_x(slot, sems, recvs, step):
        return send(slot, slot, sems.at[step], recvs.at[step], me + 1 - 2 * x, core)

    def to_y(slot, sems, recvs, step):
        return send(slot, slot, sems.at[step], recvs.at[step], me, 1 - core)

    def spread_k(step):
        slot = k_all.at[from_plane(step) * PLANE + mine]
        return (to_x(slot, xk_send, xk_recv, step), to_y(slot, yk_send, yk_recv, step))

    def spread_v(step):
        slot = v_all.at[from_plane(step) * PLANE + mine]
        return (to_x(slot, xv_send, xv_recv, step), to_y(slot, yv_send, yv_recv, step))

    def relay_k(step):
        return (to_y(k_all.at[x_block(step)], fk_send, fk_recv, step),)

    def relay_v(step):
        return (to_y(v_all.at[x_block(step)], fv_send, fv_recv, step),)

    def start(copies):
        for copy in copies:
            copy.start()

    def forward(step):
        source = from_plane(step)
        with scope(f"zk#s={step}"):
            arrived(k_all.at[source * PLANE + mine], zk_recv.at[source])
        start(spread_k(step))
        with scope(f"zv#s={step}"):
            arrived(v_all.at[source * PLANE + mine], zv_recv.at[source])
        start(spread_v(step))

    def relay(step):
        with scope(f"rk#s={step}"):
            arrived(k_all.at[x_block(step)], xk_recv.at[step])
        start(relay_k(step))
        with scope(f"rv#s={step}"):
            arrived(v_all.at[x_block(step)], xv_recv.at[step])
        start(relay_v(step))

    def ready(step):
        far = from_plane(step) * PLANE + (PLANE - 1 - mine)
        with scope(f"ready#s={step}"):
            arrived(k_all.at[y_block(step)], yk_recv.at[step])
            arrived(v_all.at[y_block(step)], yv_recv.at[step])
            arrived(k_all.at[far], fk_recv.at[step])
            arrived(v_all.at[far], fv_recv.at[step])

    def ready_q(step):
        with scope(f"q#s={step}"):
            slot = q_all.at[from_plane(step)]
            arrived(slot, q_recv.at[from_plane(step)])

    with scope("w_hid"):
        loads[0].wait()
    with scope("w_k"):
        loads[1].wait()
        loads[2].wait()
    with scope("p_k"):
        first = project(wk1).astype(jnp.bfloat16)
        second = project(wk2).astype(jnp.bfloat16)

        def put_k(head, value):
            k_out[head] = value

        joined(first, second, put_k)

        @pl.when(home)
        def _():
            k_all[me] = k_out[plane]

    with scope("barrier"):
        pl.semaphore_wait(barrier, groups - 1 + 2 + jnp.where(away, 1, 0))
    pl.when(home)(lambda: start(spread_k(0)))
    moment("k")
    with scope("w_v"):
        loads[3].wait()
    with scope("p_v"):
        value = project(wv).astype(jnp.bfloat16)
        for head in range(groups):
            v_out[head] = value[:, head * head_v : (head + 1) * head_v]

        @pl.when(home)
        def _():
            v_all[me] = v_out[plane]

    pl.when(home)(lambda: start(spread_v(0)))
    moment("v")
    with scope("w_q"):
        loads[4].wait()
        loads[5].wait()
    with scope("p_q"):
        first = (project(wq1) * score_scale).astype(jnp.bfloat16)
        second = (project(wq2) * score_scale).astype(jnp.bfloat16)

        def put_q(head, value):
            q_out[head] = value

        joined(first, second, put_q)

        @pl.when(home)
        def _():
            q_all[plane] = q_out[plane]

    moment("q")
    loads[6].wait()
    wo_copy = send(wo.at[core], wo.at[core], wo_send, wo_recv, me, 1 - core)
    wo_copy.start()
    loads[7].wait()
    loads[8].wait()
    for head in range(groups):
        lam_all[core, head] = jnp.full(lam_all.shape[2:], lam_ref[head], jnp.float32)
    lam_copy = send(lam_all.at[core], lam_all.at[core], lam_send, lam_recv, me, 1 - core)
    lam_copy.start()

    tile = ROW_TILE
    tiles = rows // tile
    chunk = PLANE * rows
    lane = lax.broadcasted_iota(jnp.int32, (tile, width), 1)

    def pair_tile(group, key_group, part, diagonal):
        begin_row = pl.multiple_of(part * tile, tile)
        queries = q_all[group, pl.ds(begin_row, tile), :]
        zero = jnp.zeros_like(queries)
        both = jnp.concatenate(
            (jnp.where(lane < qk, queries, zero), jnp.where(lane >= qk, queries, zero)), axis=0
        )
        keys = k_all[pl.ds(key_group * PLANE, PLANE)].reshape(chunk, width)
        values = v_all[pl.ds(key_group * PLANE, PLANE)].reshape(chunk, head_v)
        scores = lax.dot_general(
            both, keys, (((1,), (1,)), ((), ())), preferred_element_type=jnp.float32
        )
        cuts = [scores[:, c * LANES : (c + 1) * LANES] for c in range(chunk // LANES)]
        if diagonal:
            row = lax.rem(lax.broadcasted_iota(jnp.int32, (2 * tile, LANES), 0), tile)
            slack = (
                mine * rows
                + begin_row
                + row
                - lax.broadcasted_iota(jnp.int32, (2 * tile, LANES), 1)
            )
            cuts = [jnp.where(slack >= c * LANES, cut, masked_score) for c, cut in enumerate(cuts)]
        highest = cuts[0]
        for cut in cuts[1:]:
            highest = jnp.maximum(highest, cut)
        running_max = max_all[group, part]
        new_max = jnp.maximum(
            running_max,
            jnp.broadcast_to(jnp.max(highest, axis=-1, keepdims=True), highest.shape),
        )
        rescale = jnp.exp2(running_max - new_max)
        weights = [jnp.exp2(cut - new_max) for cut in cuts]
        new_sum = weights[0]
        for weight in weights[1:]:
            new_sum = new_sum + weight
        accum = jnp.dot(
            jnp.concatenate([weight.astype(jnp.bfloat16) for weight in weights], axis=1),
            values,
            preferred_element_type=jnp.float32,
        )
        max_all[group, part] = new_max
        sum_all[group, part] = sum_all[group, part] * rescale + new_sum
        acc_all[group, part] = acc_all[group, part] * rescale + accum

    def pair(group, key_group, diagonal):
        if not COMPUTE:
            return
        with scope("pair_d" if diagonal else "pair"):
            lax.fori_loop(
                0, tiles, lambda t, c: (pair_tile(group, key_group, t, diagonal), c)[1], 0
            )

    def meet(step, earlier):
        one, other = from_plane(step), from_plane(earlier)
        pair(jnp.maximum(one, other), jnp.minimum(one, other), False)

    def normed_copy(group):
        return send(
            n_out.at[group],
            n_all.at[y, plane],
            n_send.at[group],
            n_recv.at[plane],
            *owner(group),
        )

    def partner_copy(head):
        slot = n_all.at[core, head]
        return send(slot, slot, r_send.at[head], r_recv.at[head], me, 1 - core)

    gain = gain_ref[...]

    def finish(step):
        group = from_plane(step)
        if not COMPUTE:
            return

        def finish_tile(part, _):
            begin_row = pl.multiple_of(part * tile, tile)
            heads_out = acc_all[group, part] / jnp.sum(
                sum_all[group, part], axis=-1, keepdims=True
            )
            mixed = heads_out[:tile] - lam_all[y, plane][:1] * heads_out[tile:]
            scale_rows = lax.rsqrt(jnp.mean(mixed * mixed, axis=-1, keepdims=True) + epsilon)
            normed = (mixed * scale_rows * gain).astype(jnp.bfloat16)
            n_out[group, pl.ds(begin_row, tile), :] = normed
            return 0

        lax.fori_loop(0, tiles, finish_tile, 0)

    def deliver(step):
        finish(step)
        group = from_plane(step)
        if step == 0:

            @pl.when(home)
            def _():
                n_all[core, plane] = n_out[plane]
                partner_copy(plane).start()

            @pl.when(away)
            def _():
                normed_copy(group).start()

        else:
            normed_copy(group).start()

    max_all[...] = jnp.full(max_all.shape, masked_score, jnp.float32)
    sum_all[...] = jnp.zeros(sum_all.shape, jnp.float32)
    acc_all[...] = jnp.zeros(acc_all.shape, jnp.float32)

    def diagonal(step):
        pair(from_plane(step), from_plane(step), True)

    moment("0")
    arrived(lam_all.at[1 - core], lam_recv)
    diagonal(0)
    moment("1")
    meet(1, 0)
    diagonal(1)

    @pl.when(lower)
    def _():
        deliver(1)
        deliver(0)

    moment("2")
    meet(2, 0)
    moment("2a")
    meet(2, 1)
    moment("2b")
    diagonal(2)

    @pl.when(jnp.logical_not(swapped))
    def _():
        deliver(2)

    moment("3")

    @pl.when(jnp.logical_not(swapped))
    def _():
        meet(3, 2)

    moment("3a")

    @pl.when(lower)
    def _():
        meet(3, 0)
        meet(3, 1)

    moment("4")

    @pl.when(jnp.logical_and(swapped, lower))
    def _():
        meet(3, 2)
        deliver(2)

    diagonal(3)
    deliver(3)

    @pl.when(jnp.logical_and(swapped, upper))
    def _():
        meet(3, 2)
        deliver(2)

    @pl.when(upper)
    def _():
        meet(3, 1)
        deliver(1)
        meet(3, 0)
        deliver(0)

    def collect(head):
        @pl.when(jnp.logical_or(plane != head, away))
        def _():
            slot = n_all.at[core, head]
            with scope(f"n#h={head}"):
                arrived(slot, n_recv.at[head])
            partner_copy(head).start()

    def out_part(tp_index, first, last):
        heads = slice(first * head_v, (first + half) * head_v)
        with scope(f"out#f={first}"):
            normed = jnp.concatenate(
                [n_all[tp_index, head] for head in range(first, first + half)], axis=1
            )

            def out_tile(index, _):
                columns = pl.ds(pl.multiple_of(index * OUT_TILE, OUT_TILE), OUT_TILE)
                part = jnp.dot(
                    normed, wo[tp_index, heads, columns], preferred_element_type=jnp.float32
                )
                if last is not None:
                    part = part + out_acc[:, columns]
                if last:
                    out_ref[:, columns] = part.astype(jnp.bfloat16)
                else:
                    out_acc[:, columns] = part
                return 0

            lax.fori_loop(0, out_ref.shape[1] // OUT_TILE, out_tile, 0)

    for first in range(0, groups, half):
        for head in range(first, first + half):
            collect(head)
        out_part(core, first, None if first == 0 else False)
    arrived(wo.at[1 - core], wo_recv)
    for first in range(0, groups, half):
        with scope(f"rrecv#f={first}"):
            for head in range(first, first + half):
                arrived(n_all.at[1 - core, head], r_recv.at[head])
        out_part(1 - core, first, first + half == groups)

    with scope("drain"):
        wo_copy.wait_send()
        lam_copy.wait_send()
        for step in range(groups):
            for copies in (spread_k, spread_v, relay_k, relay_v):
                for copy in copies(step):
                    copy.wait_send()

        @pl.when(away)
        def _():
            z_done(("k", 0), ("v", 0), ("q", 0))
            normed_copy(plane).wait_send()

        for step in range(1, groups):
            z_done(("k", step), ("v", step), ("q", step))
            normed_copy(from_plane(step)).wait_send()
        for head in range(groups):
            partner_copy(head).wait_send()


COMPUTE = True
ORDER = (
    {"k": "k1", "v": "v1k2v2k3v3", "q": "q1", "0": "r0z1w0", "1": "z2r1w1q2q3a1", "2": "z3r2a2", "2b": "w2r3", "3": "a3", "4": "w3"},
    {"k": "k0", "v": "v0k1v1k2v2k3v3", "q": "q0q1", "0": "z0z1r0w0a0", "1": "z2r1w1q2q3a1", "2": "z3r2a2", "2b": "w2r3", "3": "a3", "4": "w3"},
    {"k": "k1k2", "v": "v1v2k3v3", "q": "q1q2q3", "0": "r0z1w0", "1": "z2r1z3w1a1", "2": "r2a2", "2b": "w2r3", "3": "a3", "4": "w3"},
    {"k": "k0", "v": "v0k1v1k2v2k3v3", "q": "q0q1q2q3", "0": "z0z1r0w0a0", "1": "z2r1z3w1a1", "2": "r2a2", "2b": "w2r3", "3": "a3", "4": "w3"},
    {"k": "k1k2", "v": "v1v2k3v3", "q": "q1q2q3", "0": "r0z1w0", "1": "z2r1z3w1a1", "2": "r2w2", "2b": "r3a2", "3": "a3", "4": "w3"},
    {"k": "k0", "v": "v0k1v1k2v2k3v3", "q": "q0q1q2q3", "0": "z0z1r0w0a0", "1": "z2r1z3w1a1", "2": "r2w2", "2b": "r3a2", "3": "a3", "4": "w3"},
    {"k": "k1", "v": "v1k2v2k3v3", "q": "q1", "0": "r0z1w0", "1": "z2r1w1q2q3a1", "2": "z3r2w2", "2b": "r3a2", "3": "a3", "4": "w3"},
    {"k": "k0", "v": "v0k1v1k2v2k3v3", "q": "q0q1", "0": "z0z1r0w0a0", "1": "z2r1w1q2q3a1", "2": "z3r2w2", "2b": "r3a2", "3": "a3", "4": "w3"},
)


def fused_shards(
    hidden_in, query_one, query_two, key_one, key_two, value_proj, lambdas, norm_gain, out_proj
):
    groups = lambdas.shape[0]
    rows, depth = hidden_in.shape
    head_qk = query_one.shape[1] // groups
    head_v = value_proj.shape[1] // groups
    width = 2 * head_qk
    blocks = groups * PLANE
    columns = out_proj.shape[1]
    score_scale = 1.75 * head_qk ** (-0.5) * math.log2(math.e)
    bf16 = jnp.bfloat16
    dma = pltpu.SemaphoreType.DMA
    hbm = pl.BlockSpec(memory_space=pltpu.HBM)
    vmem = pl.BlockSpec(memory_space=pltpu.VMEM)

    def body(*refs):
        fused_kernel(groups, score_scale, *refs)

    return pl.pallas_call(
        body,
        name="fused_attention",
        out_shape=jax.ShapeDtypeStruct((rows, columns), bf16),
        in_specs=[hbm] * 9,
        out_specs=vmem,
        scratch_shapes=[
            pltpu.VMEM(hidden_in.shape, bf16),
            pltpu.VMEM(query_one.shape, bf16),
            pltpu.VMEM(query_two.shape, bf16),
            pltpu.VMEM(key_one.shape, bf16),
            pltpu.VMEM(key_two.shape, bf16),
            pltpu.VMEM(value_proj.shape, bf16),
            pltpu.VMEM((2,) + out_proj.shape, bf16),
            pltpu.SMEM(lambdas.shape, jnp.float32),
            pltpu.VMEM((2, groups, 8, head_v), jnp.float32),
            pltpu.VMEM((1, head_v), jnp.float32),
            pltpu.VMEM((groups, rows, width), bf16),
            pltpu.VMEM((groups, rows, head_v), bf16),
            pltpu.VMEM((groups, rows, width), bf16),
            pltpu.VMEM((blocks, rows, width), bf16),
            pltpu.VMEM((blocks, rows, head_v), bf16),
            pltpu.VMEM((groups, rows, width), bf16),
            pltpu.VMEM((groups, rows, head_v), bf16),
            pltpu.VMEM((2, groups, rows, head_v), bf16),
            pltpu.VMEM((groups, rows // ROW_TILE, 2 * ROW_TILE, LANES), jnp.float32),
            pltpu.VMEM((groups, rows // ROW_TILE, 2 * ROW_TILE, LANES), jnp.float32),
            pltpu.VMEM((groups, rows // ROW_TILE, 2 * ROW_TILE, head_v), jnp.float32),
            pltpu.VMEM((rows, columns), jnp.float32),
            dma((9,)),
            dma,
            dma,
            dma,
            dma,
        ]
        + [dma((groups,))] * 22,
        compiler_params=pltpu.CompilerParams(
            collective_id=0, has_side_effects=True, vmem_limit_bytes=VMEM_LIMIT
        ),
    )(
        *(
            pltpu.with_memory_space_constraint(item, pltpu.HBM)
            for item in (
                hidden_in,
                query_one,
                query_two,
                key_one,
                key_two,
                value_proj,
                lambdas,
                norm_gain.reshape(1, head_v),
                out_proj,
            )
        )
    )


VMEM_LIMIT = 48 * 1024 * 1024


def solution(mesh):
    placed = (
        P("sp", None),
        P(None, "tp"),
        P(None, "tp"),
        P(None, "tp"),
        P(None, "tp"),
        P(None, "tp"),
        P("tp"),
        P(),
        P("tp", None),
    )

    def body(*args):
        groups = args[6].shape[0]
        split = groups * PLANE == mesh.shape["sp"] and mesh.shape["tp"] == 2
        return (fused_shards if split else shards)(*args)

    return jax.shard_map(
        body, mesh=mesh, in_specs=placed, out_specs=P("sp", None), check_vma=False
    )
```

```python
import functools
import math

import jax
import jax.numpy as jnp
from jax import lax
from jax.experimental import pallas as pl
from jax.experimental.pallas import tpu as pltpu
from jax.sharding import PartitionSpec as P

epsilon = 1e-06
masked_score = -1e30


def shards(
    hidden_in, query_one, query_two, key_one, key_two, value_proj, lambdas, norm_gain, out_proj
):
    heads_dev = lambdas.shape[0]
    head_qk = query_one.shape[1] // heads_dev
    head_v = value_proj.shape[1] // heads_dev
    width_q = heads_dev * head_qk
    score_scale = 1.75 * head_qk ** (-0.5)
    joined = jnp.concatenate((query_one, query_two, key_one, key_two, value_proj), axis=1)
    projected = jnp.dot(hidden_in, joined, preferred_element_type=jnp.float32).astype(jnp.bfloat16)
    tok_rows = projected.shape[0]
    key_values = projected[:, 2 * width_q :]
    my_index = lax.axis_index("sp")
    offset = my_index * tok_rows
    query_sets = (projected[:, : 2 * width_q],)
    position_sets = (offset + jnp.arange(tok_rows, dtype=jnp.int32),)
    groups = []
    for query_rows, positions in zip(query_sets, position_sets):
        group_rows = query_rows.shape[0]
        query_a = query_rows[:, :width_q].reshape(group_rows, heads_dev, head_qk)
        query_b = query_rows[:, width_q:].reshape(group_rows, heads_dev, head_qk)
        groups.append((query_a, query_b, positions, positions[group_rows - 1]))

    def one_map(queries, keys, value_rows, allowed, running_max, running_sum, accum):
        scores = (
            jnp.einsum("qhd,khd->hqk", queries, keys, preferred_element_type=jnp.float32)
            * score_scale
        )
        scores = jnp.where(allowed[None], scores, masked_score)
        new_max = jnp.maximum(running_max, jnp.max(scores, axis=-1))
        rescale = jnp.exp(running_max - new_max)
        weights = jnp.where(allowed[None], jnp.exp(scores - new_max[..., None]), 0.0)
        new_sum = running_sum * rescale + jnp.sum(weights, axis=-1)
        added = jnp.einsum(
            "hqk,khe->hqe",
            weights.astype(jnp.bfloat16),
            value_rows,
            preferred_element_type=jnp.float32,
        )
        return (new_max, new_sum, accum * rescale[..., None] + added)

    def absorb(group_state, group, kblock, kstart):
        query_a, query_b, positions, last_pos = group
        block_rows = kblock.shape[0]
        k_pos = kstart + jnp.arange(block_rows, dtype=jnp.int32)
        allowed = k_pos[None, :] <= positions[:, None]
        keys_a = kblock[:, :width_q].reshape(block_rows, heads_dev, head_qk)
        keys_b = kblock[:, width_q : 2 * width_q].reshape(block_rows, heads_dev, head_qk)
        value_rows = kblock[:, 2 * width_q :].reshape(block_rows, heads_dev, head_v)
        first_map = one_map(query_a, keys_a, value_rows, allowed, *group_state[:3])
        second_map = one_map(query_b, keys_b, value_rows, allowed, *group_state[3:])
        return first_map + second_map

    group = groups[0]
    group_rows = group[0].shape[0]
    start_max = jnp.full((heads_dev, group_rows), masked_score, jnp.float32)
    start_sum = jnp.zeros((heads_dev, group_rows), jnp.float32)
    start_acc = jnp.zeros((heads_dev, group_rows, head_v), jnp.float32)
    initial_list = [(start_max, start_sum, start_acc, start_max, start_sum, start_acc)]
    initial = tuple(initial_list)
    softmax_state = initial
    kv_piece = lax.all_gather(key_values, "sp", axis=0, tiled=True)
    piece_rows = kv_piece.shape[0]
    block_rows = math.gcd(piece_rows, 512)
    block_count = piece_rows // block_rows
    stacked = kv_piece.reshape(block_count, block_rows, kv_piece.shape[1])

    def absorb_step(carried, blocks_in):
        kblock, block_index = blocks_in
        kstart = block_index * block_rows
        renewed = []
        for group, group_state in zip(groups, carried):
            renewed.append(
                lax.cond(
                    kstart <= group[3],
                    lambda inner, group=group: absorb(inner, group, kblock, kstart),
                    lambda inner: inner,
                    group_state,
                )
            )
        return (tuple(renewed), None)

    softmax_state, _ = lax.scan(
        absorb_step, softmax_state, (stacked, jnp.arange(block_count, dtype=jnp.int32))
    )
    normed_sets = []
    for group_state in softmax_state:
        out_a = group_state[2] / group_state[1][..., None]
        out_b = group_state[5] / group_state[4][..., None]
        mixed_out = out_a - lambdas[:, None, None] * out_b
        scale_rows = lax.rsqrt(jnp.mean(mixed_out * mixed_out, axis=-1, keepdims=True) + epsilon)
        normed = (mixed_out * scale_rows * norm_gain).astype(jnp.bfloat16)
        group_rows = normed.shape[1]
        normed_sets.append(jnp.transpose(normed, (1, 0, 2)).reshape(group_rows, heads_dev * head_v))
    normed_all = normed_sets[0]
    partial_value = jnp.dot(normed_all, out_proj, preferred_element_type=jnp.float32)
    result = lax.psum(partial_value.astype(jnp.bfloat16), "tp")
    return result


MESH = pl.DeviceIdType.MESH
PLANE = 4
ROW_TILE = 256
OUT_TILE = 2048
LANES = 128


def fused_kernel(
    groups,
    score_scale,
    hidden_hbm,
    q1_hbm,
    q2_hbm,
    k1_hbm,
    k2_hbm,
    v_hbm,
    lam_hbm,
    gain_hbm,
    wo_hbm,
    out_ref,
    hid,
    wq1,
    wq2,
    wk1,
    wk2,
    wv,
    wo,
    lam_ref,
    lam_all,
    gain_ref,
    k_out,
    v_out,
    q_out,
    k_all,
    v_all,
    q_all,
    n_out,
    n_all,
    max_all,
    sum_all,
    acc_all,
    out_acc,
    load_sem,
    sent,
    wo_sent,
    wo_recv,
    lam_sent,
    lam_recv,
    zk_recv,
    zv_recv,
    q_recv,
    xk_recv,
    xv_recv,
    y_recv,
    n_recv,
    r_recv,
):
    scope = jax.named_scope
    me = lax.axis_index("sp")
    core = lax.axis_index("tp")
    plane = me // PLANE
    spot = lax.rem(me, PLANE)
    x = lax.rem(spot, 2)
    y = spot // 2
    mine = 2 * core + x
    home = core == y
    away = core != y
    rows = hid.shape[0]
    qk = q1_hbm.shape[1] // groups
    width = 2 * qk
    head_v = v_hbm.shape[1] // groups

    def load(index, src, dst):
        return pltpu.make_async_copy(src, dst, load_sem.at[index])

    depth = hid.shape[1]
    cut = depth // K_CUTS
    cuts = [slice(index * cut, (index + 1) * cut) for index in range(K_CUTS)]
    loads = []
    for index, part in enumerate(cuts):
        loads += [
            load(index, hidden_hbm.at[:, part], hid.at[:, part]),
            load(index, k1_hbm.at[part], wk1.at[part]),
            load(index, k2_hbm.at[part], wk2.at[part]),
        ]
    loads += [
        load(K_CUTS, v_hbm, wv),
        load(K_CUTS + 1, q1_hbm, wq1),
        load(K_CUTS + 1, q2_hbm, wq2),
        load(K_CUTS + 2, wo_hbm, wo.at[core]),
        load(K_CUTS + 3, lam_hbm, lam_ref),
        load(K_CUTS + 4, gain_hbm, gain_ref),
    ]
    for item in loads:
        item.start()

    def loaded(index, ref):
        pltpu.make_async_copy(ref, ref, load_sem.at[index]).wait()

    barrier = pltpu.get_barrier_semaphore()

    def greet(index, tp_index):
        pl.semaphore_signal(barrier, inc=1, device_id=(index, tp_index), device_id_type=MESH)

    def owner(index):
        return index * PLANE + mine, y

    for step in range(1, groups):
        greet(*owner(lax.rem(plane + step, groups)))
    pl.when(away)(lambda: greet(*owner(plane)))
    greet(me, 1 - core)
    greet(me + 1 - 2 * x, core)

    def send(src, dst, recv_sem, index, tp_index, send_sem=None):
        return pltpu.make_async_remote_copy(
            src_ref=src,
            dst_ref=dst,
            send_sem=sent if send_sem is None else send_sem,
            recv_sem=recv_sem,
            device_id=(index, tp_index),
            device_id_type=MESH,
        )

    def arrived(ref, recv_sem):
        pltpu.make_async_copy(ref, ref, recv_sem).wait()

    half = groups // 2
    upper = plane >= half
    lower = jnp.logical_not(upper)
    base = jnp.where(upper, half, 0)
    swapped = lax.rem(plane, half) == 0

    def from_plane(step):
        if step < half:
            return base + lax.rem(plane + step, half)
        return (half - base) + jnp.where(swapped, groups - 1 - step, step - half)

    def project(weight_ref):
        return jnp.dot(hid[...], weight_ref[...], preferred_element_type=jnp.float32)

    def joined(first, second, store):
        for head in range(groups):
            cut = slice(head * qk, (head + 1) * qk)
            store(head, jnp.concatenate((first[:, cut], second[:, cut]), axis=1))

    def z_copy(kind, step):
        target = from_plane(step)
        out, full, recvs = {
            "k": (k_out, k_all.at[me], zk_recv),
            "v": (v_out, v_all.at[me], zv_recv),
            "q": (q_out, q_all.at[plane], q_recv),
        }[kind]
        return send(
            out.at[target],
            full,
            recvs.at[plane],
            *owner(target),
        )

    def z_start(*items):
        for kind, step in items:
            z_copy(kind, step).start()

    def perform(items):
        for item in items:
            kind, step = item[0], int(item[1])
            if kind in "kvq":
                z_copy(kind, step).start()
            else:
                {"z": forward, "r": relay, "w": ready, "a": ready_q}[kind](step)

    places = [
        jnp.logical_and(plane == index, place) for index in range(groups) for place in (home, away)
    ]

    def moment(name):
        texts = [order.get(name, "") for order in ORDER]
        lists = [[text[i : i + 2] for i in range(0, len(text), 2)] for text in texts]
        if all(items == lists[0] for items in lists):
            perform(lists[0])
            return
        for items in dict.fromkeys(map(tuple, lists)):
            if items:
                place = functools.reduce(
                    jnp.logical_or, [p for p, other in zip(places, lists) if tuple(other) == items]
                )
                pl.when(place)(lambda items=items: perform(items))

    def x_block(step):
        return from_plane(step) * PLANE + mine + 1 - 2 * x

    def y_block(step):
        return from_plane(step) * PLANE + mine + 2 - 4 * core

    def to_x(slot, recvs, step):
        return send(slot, slot, recvs.at[step], me + 1 - 2 * x, core)

    def to_y(slot, step):
        return send(slot, slot, y_recv.at[step], me, 1 - core)

    def spread_k(step):
        slot = k_all.at[from_plane(step) * PLANE + mine]
        return (to_x(slot, xk_recv, step), to_y(slot, step))

    def spread_v(step):
        slot = v_all.at[from_plane(step) * PLANE + mine]
        return (to_x(slot, xv_recv, step), to_y(slot, step))

    def relay_k(step):
        return (to_y(k_all.at[x_block(step)], step),)

    def relay_v(step):
        return (to_y(v_all.at[x_block(step)], step),)

    def start(copies):
        for copy in copies:
            copy.start()

    def forward(step):
        source = from_plane(step)
        with scope(f"zk#s={step}"):
            arrived(k_all.at[source * PLANE + mine], zk_recv.at[source])
        start(spread_k(step))
        with scope(f"zv#s={step}"):
            arrived(v_all.at[source * PLANE + mine], zv_recv.at[source])
        start(spread_v(step))

    def relay(step):
        with scope(f"rk#s={step}"):
            arrived(k_all.at[x_block(step)], xk_recv.at[step])
        start(relay_k(step))
        with scope(f"rv#s={step}"):
            arrived(v_all.at[x_block(step)], xv_recv.at[step])
        start(relay_v(step))

    def ready(step):
        with scope(f"ready#s={step}"):
            arrived(k_all.at[pl.ds(0, 4)], y_recv.at[step])

    def ready_q(step):
        with scope(f"q#s={step}"):
            slot = q_all.at[from_plane(step)]
            arrived(slot, q_recv.at[from_plane(step)])

    with scope("p_k"):
        first = second = None
        for index, part in enumerate(cuts):
            with scope(f"w_k#{index}"):
                loaded(index, wv.at[pl.ds(0, cut * (rows + 2 * wk1.shape[1]) // wv.shape[1])])
            more = [
                jnp.dot(hid[:, part], weight[part], preferred_element_type=jnp.float32)
                for weight in (wk1, wk2)
            ]
            first = more[0] if first is None else first + more[0]
            second = more[1] if second is None else second + more[1]
        first = first.astype(jnp.bfloat16)
        second = second.astype(jnp.bfloat16)

        def put_k(head, value):
            k_out[head] = value

        joined(first, second, put_k)

        @pl.when(home)
        def _():
            k_all[me] = k_out[plane]

    with scope("barrier"):
        pl.semaphore_wait(barrier, groups - 1 + 2 + jnp.where(away, 1, 0))
    pl.when(home)(lambda: start(spread_k(0)))
    moment("k")
    with scope("w_v"):
        loaded(K_CUTS, wv)
    with scope("p_v"):
        value = project(wv).astype(jnp.bfloat16)
        for head in range(groups):
            v_out[head] = value[:, head * head_v : (head + 1) * head_v]

        @pl.when(home)
        def _():
            v_all[me] = v_out[plane]

    pl.when(home)(lambda: start(spread_v(0)))
    moment("v")
    with scope("w_q"):
        loaded(K_CUTS + 1, wv)
    with scope("p_q"):
        first = (project(wq1) * score_scale).astype(jnp.bfloat16)
        second = (project(wq2) * score_scale).astype(jnp.bfloat16)

        def put_q(head, value):
            q_out[head] = value

        joined(first, second, put_q)

        @pl.when(home)
        def _():
            q_all[plane] = q_out[plane]

    moment("q")
    loaded(K_CUTS + 2, wo.at[core])
    wo_copy = send(wo.at[core], wo.at[core], wo_recv, me, 1 - core, wo_sent)
    wo_copy.start()
    loads[-2].wait()
    loads[-1].wait()
    for head in range(groups):
        lam_all[core, head] = jnp.full(lam_all.shape[2:], lam_ref[head], jnp.float32)
    lam_copy = send(lam_all.at[core], lam_all.at[core], lam_recv, me, 1 - core, lam_sent)
    lam_copy.start()

    tile = ROW_TILE
    tiles = rows // tile
    chunk = PLANE * rows
    lane = lax.broadcasted_iota(jnp.int32, (tile, width), 1)

    def pair_tile(group, key_group, part, diagonal):
        begin_row = pl.multiple_of(part * tile, tile)
        queries = q_all[group, pl.ds(begin_row, tile), :]
        zero = jnp.zeros_like(queries)
        both = jnp.concatenate(
            (jnp.where(lane < qk, queries, zero), jnp.where(lane >= qk, queries, zero)), axis=0
        )
        keys = k_all[pl.ds(key_group * PLANE, PLANE)].reshape(chunk, width)
        values = v_all[pl.ds(key_group * PLANE, PLANE)].reshape(chunk, head_v)
        scores = lax.dot_general(
            both, keys, (((1,), (1,)), ((), ())), preferred_element_type=jnp.float32
        )
        cuts = [scores[:, c * LANES : (c + 1) * LANES] for c in range(chunk // LANES)]
        if diagonal:
            row = lax.rem(lax.broadcasted_iota(jnp.int32, (2 * tile, LANES), 0), tile)
            slack = (
                mine * rows
                + begin_row
                + row
                - lax.broadcasted_iota(jnp.int32, (2 * tile, LANES), 1)
            )
            cuts = [jnp.where(slack >= c * LANES, cut, masked_score) for c, cut in enumerate(cuts)]
        highest = cuts[0]
        for cut in cuts[1:]:
            highest = jnp.maximum(highest, cut)
        running_max = max_all[group, part]
        new_max = jnp.maximum(
            running_max,
            jnp.broadcast_to(jnp.max(highest, axis=-1, keepdims=True), highest.shape),
        )
        rescale = jnp.exp2(running_max - new_max)
        weights = [jnp.exp2(cut - new_max) for cut in cuts]
        new_sum = weights[0]
        for weight in weights[1:]:
            new_sum = new_sum + weight
        accum = jnp.dot(
            jnp.concatenate([weight.astype(jnp.bfloat16) for weight in weights], axis=1),
            values,
            preferred_element_type=jnp.float32,
        )
        max_all[group, part] = new_max
        sum_all[group, part] = sum_all[group, part] * rescale + new_sum
        acc_all[group, part] = acc_all[group, part] * rescale + accum

    def pair(group, key_group, diagonal):
        if not COMPUTE:
            return
        with scope("pair_d" if diagonal else "pair"):
            lax.fori_loop(
                0, tiles, lambda t, c: (pair_tile(group, key_group, t, diagonal), c)[1], 0
            )

    def meet(step, earlier):
        one, other = from_plane(step), from_plane(earlier)
        pair(jnp.maximum(one, other), jnp.minimum(one, other), False)

    def normed_copy(group):
        return send(
            n_out.at[group],
            n_all.at[y, plane],
            n_recv.at[plane],
            *owner(group),
        )

    def partner_copy(head):
        slot = n_all.at[core, head]
        return send(slot, slot, r_recv.at[head // half], me, 1 - core)

    gain = gain_ref[...]

    def finish(step):
        group = from_plane(step)
        if not COMPUTE:
            return

        def finish_tile(part, _):
            begin_row = pl.multiple_of(part * tile, tile)
            heads_out = acc_all[group, part] / jnp.sum(
                sum_all[group, part], axis=-1, keepdims=True
            )
            mixed = heads_out[:tile] - lam_all[y, plane][:1] * heads_out[tile:]
            scale_rows = lax.rsqrt(jnp.mean(mixed * mixed, axis=-1, keepdims=True) + epsilon)
            normed = (mixed * scale_rows * gain).astype(jnp.bfloat16)
            n_out[group, pl.ds(begin_row, tile), :] = normed
            return 0

        lax.fori_loop(0, tiles, finish_tile, 0)

    def deliver(step):
        finish(step)
        group = from_plane(step)
        if step == 0:

            @pl.when(home)
            def _():
                n_all[core, plane] = n_out[plane]
                partner_copy(plane).start()

            @pl.when(away)
            def _():
                normed_copy(group).start()

        else:
            normed_copy(group).start()

    max_all[...] = jnp.full(max_all.shape, masked_score, jnp.float32)
    sum_all[...] = jnp.zeros(sum_all.shape, jnp.float32)
    acc_all[...] = jnp.zeros(acc_all.shape, jnp.float32)

    def diagonal(step):
        pair(from_plane(step), from_plane(step), True)

    moment("0")
    arrived(lam_all.at[1 - core], lam_recv)
    diagonal(0)
    moment("1")
    meet(1, 0)
    diagonal(1)

    @pl.when(lower)
    def _():
        deliver(1)
        deliver(0)

    moment("2")
    meet(2, 0)
    moment("2a")
    meet(2, 1)
    moment("2b")
    diagonal(2)

    @pl.when(jnp.logical_not(swapped))
    def _():
        deliver(2)

    moment("3")

    @pl.when(jnp.logical_not(swapped))
    def _():
        meet(3, 2)

    moment("3a")

    @pl.when(lower)
    def _():
        meet(3, 0)
        meet(3, 1)

    moment("4")

    @pl.when(jnp.logical_and(swapped, lower))
    def _():
        meet(3, 2)
        deliver(2)

    diagonal(3)
    deliver(3)

    @pl.when(jnp.logical_and(swapped, upper))
    def _():
        meet(3, 2)
        deliver(2)

    @pl.when(upper)
    def _():
        meet(3, 1)
        deliver(1)
        meet(3, 0)
        deliver(0)

    def collect(head):
        @pl.when(jnp.logical_or(plane != head, away))
        def _():
            slot = n_all.at[core, head]
            with scope(f"n#h={head}"):
                arrived(slot, n_recv.at[head])
            partner_copy(head).start()

    def out_part(tp_index, first, last):
        heads = slice(first * head_v, (first + half) * head_v)
        with scope(f"out#f={first}"):
            normed = jnp.concatenate(
                [n_all[tp_index, head] for head in range(first, first + half)], axis=1
            )

            def out_tile(index, _):
                columns = pl.ds(pl.multiple_of(index * OUT_TILE, OUT_TILE), OUT_TILE)
                part = jnp.dot(
                    normed, wo[tp_index, heads, columns], preferred_element_type=jnp.float32
                )
                if last is not None:
                    part = part + out_acc[:, columns]
                if last:
                    out_ref[:, columns] = part.astype(jnp.bfloat16)
                else:
                    out_acc[:, columns] = part
                return 0

            lax.fori_loop(0, out_ref.shape[1] // OUT_TILE, out_tile, 0)

    for first in range(0, groups, half):
        for head in range(first, first + half):
            collect(head)
        out_part(core, first, None if first == 0 else False)
    arrived(wo.at[1 - core], wo_recv)
    for first in range(0, groups, half):
        with scope(f"rrecv#f={first}"):
            arrived(n_all.at[1 - core, pl.ds(first, half)], r_recv.at[first // half])
        out_part(1 - core, first, first + half == groups)

    with scope("drain"):
        wo_copy.wait_send()
        lam_copy.wait_send()
        unit = rows * width // (2 * wo.shape[2])
        for place, extra in ((home, 0), (away, 4)):
            blocks = (groups - 1) * 4 + 6 * groups + groups + extra

            @pl.when(place)
            def _():
                arrived(wo.at[:, pl.ds(0, blocks * unit)], sent)


K_CUTS = 4
COMPUTE = True
ORDER = (
    {"k": "k1", "v": "v1k2v2k3v3", "q": "q1", "0": "r0z1w0", "1": "z2r1w1q2q3a1", "2": "z3r2a2", "2b": "w2r3", "3": "a3", "4": "w3"},
    {"k": "k0", "v": "v0k1v1k2v2k3v3", "q": "q0q1", "0": "z0z1r0w0a0", "1": "z2r1w1q2q3a1", "2": "z3r2a2", "2b": "w2r3", "3": "a3", "4": "w3"},
    {"k": "k1k2", "v": "v1v2k3v3", "q": "q1q2q3", "0": "r0z1w0", "1": "z2r1z3w1a1", "2": "r2a2", "2b": "w2r3", "3": "a3", "4": "w3"},
    {"k": "k0", "v": "v0k1v1k2v2k3v3", "q": "q0q1q2q3", "0": "z0z1r0w0a0", "1": "z2r1z3w1a1", "2": "r2a2", "2b": "w2r3", "3": "a3", "4": "w3"},
    {"k": "k1k2", "v": "v1v2k3v3", "q": "q1q2q3", "0": "r0z1w0", "1": "z2r1z3w1a1", "2": "r2w2", "2b": "r3a2", "3": "a3", "4": "w3"},
    {"k": "k0", "v": "v0k1v1k2v2k3v3", "q": "q0q1q2q3", "0": "z0z1r0w0a0", "1": "z2r1z3w1a1", "2": "r2w2", "2b": "r3a2", "3": "a3", "4": "w3"},
    {"k": "k1", "v": "v1k2v2k3v3", "q": "q1", "0": "r0z1w0", "1": "z2r1w1q2q3a1", "2": "z3r2w2", "2b": "r3a2", "3": "a3", "4": "w3"},
    {"k": "k0", "v": "v0k1v1k2v2k3v3", "q": "q0q1", "0": "z0z1r0w0a0", "1": "z2r1w1q2q3a1", "2": "z3r2w2", "2b": "r3a2", "3": "a3", "4": "w3"},
)


def fused_shards(
    hidden_in, query_one, query_two, key_one, key_two, value_proj, lambdas, norm_gain, out_proj
):
    groups = lambdas.shape[0]
    rows, depth = hidden_in.shape
    head_qk = query_one.shape[1] // groups
    head_v = value_proj.shape[1] // groups
    width = 2 * head_qk
    blocks = groups * PLANE
    columns = out_proj.shape[1]
    score_scale = 1.75 * head_qk ** (-0.5) * math.log2(math.e)
    bf16 = jnp.bfloat16
    dma = pltpu.SemaphoreType.DMA
    hbm = pl.BlockSpec(memory_space=pltpu.HBM)
    vmem = pl.BlockSpec(memory_space=pltpu.VMEM)

    def body(*refs):
        fused_kernel(groups, score_scale, *refs)

    return pl.pallas_call(
        body,
        name="fused_attention",
        out_shape=jax.ShapeDtypeStruct((rows, columns), bf16),
        in_specs=[hbm] * 9,
        out_specs=vmem,
        scratch_shapes=[
            pltpu.VMEM(hidden_in.shape, bf16),
            pltpu.VMEM(query_one.shape, bf16),
            pltpu.VMEM(query_two.shape, bf16),
            pltpu.VMEM(key_one.shape, bf16),
            pltpu.VMEM(key_two.shape, bf16),
            pltpu.VMEM(value_proj.shape, bf16),
            pltpu.VMEM((2,) + out_proj.shape, bf16),
            pltpu.SMEM(lambdas.shape, jnp.float32),
            pltpu.VMEM((2, groups, 8, head_v), jnp.float32),
            pltpu.VMEM((1, head_v), jnp.float32),
            pltpu.VMEM((groups, rows, width), bf16),
            pltpu.VMEM((groups, rows, head_v), bf16),
            pltpu.VMEM((groups, rows, width), bf16),
            pltpu.VMEM((blocks, rows, width), bf16),
            pltpu.VMEM((blocks, rows, head_v), bf16),
            pltpu.VMEM((groups, rows, width), bf16),
            pltpu.VMEM((groups, rows, head_v), bf16),
            pltpu.VMEM((2, groups, rows, head_v), bf16),
            pltpu.VMEM((groups, rows // ROW_TILE, 2 * ROW_TILE, LANES), jnp.float32),
            pltpu.VMEM((groups, rows // ROW_TILE, 2 * ROW_TILE, LANES), jnp.float32),
            pltpu.VMEM((groups, rows // ROW_TILE, 2 * ROW_TILE, head_v), jnp.float32),
            pltpu.VMEM((rows, columns), jnp.float32),
            dma((K_CUTS + 5,)),
            dma,
            dma,
            dma,
            dma,
            dma,
        ]
        + [dma((groups,))] * 7
        + [dma((2,))],
        compiler_params=pltpu.CompilerParams(
            collective_id=0, has_side_effects=True, vmem_limit_bytes=VMEM_LIMIT
        ),
    )(
        *(
            pltpu.with_memory_space_constraint(item, pltpu.HBM)
            for item in (
                hidden_in,
                query_one,
                query_two,
                key_one,
                key_two,
                value_proj,
                lambdas,
                norm_gain.reshape(1, head_v),
                out_proj,
            )
        )
    )


VMEM_LIMIT = 48 * 1024 * 1024


def solution(mesh):
    placed = (
        P("sp", None),
        P(None, "tp"),
        P(None, "tp"),
        P(None, "tp"),
        P(None, "tp"),
        P(None, "tp"),
        P("tp"),
        P(),
        P("tp", None),
    )

    def body(*args):
        groups = args[6].shape[0]
        split = groups * PLANE == mesh.shape["sp"] and mesh.shape["tp"] == 2
        return (fused_shards if split else shards)(*args)

    return jax.shard_map(
        body, mesh=mesh, in_specs=placed, out_specs=P("sp", None), check_vma=False
    )
```

```python
import functools
import math

import jax
import jax.numpy as jnp
from jax import lax
from jax.experimental import pallas as pl
from jax.experimental.pallas import tpu as pltpu
from jax.sharding import PartitionSpec as P

epsilon = 1e-06
masked_score = -1e30


def shards(
    hidden_in, query_one, query_two, key_one, key_two, value_proj, lambdas, norm_gain, out_proj
):
    heads_dev = lambdas.shape[0]
    head_qk = query_one.shape[1] // heads_dev
    head_v = value_proj.shape[1] // heads_dev
    width_q = heads_dev * head_qk
    score_scale = 1.75 * head_qk ** (-0.5)
    joined = jnp.concatenate((query_one, query_two, key_one, key_two, value_proj), axis=1)
    projected = jnp.dot(hidden_in, joined, preferred_element_type=jnp.float32).astype(jnp.bfloat16)
    tok_rows = projected.shape[0]
    key_values = projected[:, 2 * width_q :]
    my_index = lax.axis_index("sp")
    offset = my_index * tok_rows
    query_sets = (projected[:, : 2 * width_q],)
    position_sets = (offset + jnp.arange(tok_rows, dtype=jnp.int32),)
    groups = []
    for query_rows, positions in zip(query_sets, position_sets):
        group_rows = query_rows.shape[0]
        query_a = query_rows[:, :width_q].reshape(group_rows, heads_dev, head_qk)
        query_b = query_rows[:, width_q:].reshape(group_rows, heads_dev, head_qk)
        groups.append((query_a, query_b, positions, positions[group_rows - 1]))

    def one_map(queries, keys, value_rows, allowed, running_max, running_sum, accum):
        scores = (
            jnp.einsum("qhd,khd->hqk", queries, keys, preferred_element_type=jnp.float32)
            * score_scale
        )
        scores = jnp.where(allowed[None], scores, masked_score)
        new_max = jnp.maximum(running_max, jnp.max(scores, axis=-1))
        rescale = jnp.exp(running_max - new_max)
        weights = jnp.where(allowed[None], jnp.exp(scores - new_max[..., None]), 0.0)
        new_sum = running_sum * rescale + jnp.sum(weights, axis=-1)
        added = jnp.einsum(
            "hqk,khe->hqe",
            weights.astype(jnp.bfloat16),
            value_rows,
            preferred_element_type=jnp.float32,
        )
        return (new_max, new_sum, accum * rescale[..., None] + added)

    def absorb(group_state, group, kblock, kstart):
        query_a, query_b, positions, last_pos = group
        block_rows = kblock.shape[0]
        k_pos = kstart + jnp.arange(block_rows, dtype=jnp.int32)
        allowed = k_pos[None, :] <= positions[:, None]
        keys_a = kblock[:, :width_q].reshape(block_rows, heads_dev, head_qk)
        keys_b = kblock[:, width_q : 2 * width_q].reshape(block_rows, heads_dev, head_qk)
        value_rows = kblock[:, 2 * width_q :].reshape(block_rows, heads_dev, head_v)
        first_map = one_map(query_a, keys_a, value_rows, allowed, *group_state[:3])
        second_map = one_map(query_b, keys_b, value_rows, allowed, *group_state[3:])
        return first_map + second_map

    group = groups[0]
    group_rows = group[0].shape[0]
    start_max = jnp.full((heads_dev, group_rows), masked_score, jnp.float32)
    start_sum = jnp.zeros((heads_dev, group_rows), jnp.float32)
    start_acc = jnp.zeros((heads_dev, group_rows, head_v), jnp.float32)
    initial_list = [(start_max, start_sum, start_acc, start_max, start_sum, start_acc)]
    initial = tuple(initial_list)
    softmax_state = initial
    kv_piece = lax.all_gather(key_values, "sp", axis=0, tiled=True)
    piece_rows = kv_piece.shape[0]
    block_rows = math.gcd(piece_rows, 512)
    block_count = piece_rows // block_rows
    stacked = kv_piece.reshape(block_count, block_rows, kv_piece.shape[1])

    def absorb_step(carried, blocks_in):
        kblock, block_index = blocks_in
        kstart = block_index * block_rows
        renewed = []
        for group, group_state in zip(groups, carried):
            renewed.append(
                lax.cond(
                    kstart <= group[3],
                    lambda inner, group=group: absorb(inner, group, kblock, kstart),
                    lambda inner: inner,
                    group_state,
                )
            )
        return (tuple(renewed), None)

    softmax_state, _ = lax.scan(
        absorb_step, softmax_state, (stacked, jnp.arange(block_count, dtype=jnp.int32))
    )
    normed_sets = []
    for group_state in softmax_state:
        out_a = group_state[2] / group_state[1][..., None]
        out_b = group_state[5] / group_state[4][..., None]
        mixed_out = out_a - lambdas[:, None, None] * out_b
        scale_rows = lax.rsqrt(jnp.mean(mixed_out * mixed_out, axis=-1, keepdims=True) + epsilon)
        normed = (mixed_out * scale_rows * norm_gain).astype(jnp.bfloat16)
        group_rows = normed.shape[1]
        normed_sets.append(jnp.transpose(normed, (1, 0, 2)).reshape(group_rows, heads_dev * head_v))
    normed_all = normed_sets[0]
    partial_value = jnp.dot(normed_all, out_proj, preferred_element_type=jnp.float32)
    result = lax.psum(partial_value.astype(jnp.bfloat16), "tp")
    return result


MESH = pl.DeviceIdType.MESH
PLANE = 4
ROW_TILE = 256
OUT_TILE = 2048
LANES = 128


def fused_kernel(
    groups,
    score_scale,
    hidden_hbm,
    q1_hbm,
    q2_hbm,
    k1_hbm,
    k2_hbm,
    v_hbm,
    lam_hbm,
    gain_hbm,
    wo_hbm,
    out_ref,
    hid,
    wq1,
    wq2,
    wk1,
    wk2,
    wv,
    wo,
    lam_ref,
    lam_all,
    gain_ref,
    k_out,
    v_out,
    q_out,
    k_all,
    v_all,
    q_all,
    n_out,
    n_all,
    max_all,
    sum_all,
    acc_all,
    out_acc,
    load_sem,
    sent,
    wo_sent,
    wo_recv,
    lam_sent,
    lam_recv,
    zk_recv,
    zv_recv,
    q_recv,
    xk_recv,
    xv_recv,
    y_recv,
    n_recv,
    r_recv,
):
    scope = jax.named_scope
    me = lax.axis_index("sp")
    core = lax.axis_index("tp")
    plane = me // PLANE
    spot = lax.rem(me, PLANE)
    x = lax.rem(spot, 2)
    y = spot // 2
    mine = 2 * core + x
    home = core == y
    away = core != y
    rows = hid.shape[0]
    qk = q1_hbm.shape[1] // groups
    width = 2 * qk
    head_v = v_hbm.shape[1] // groups

    def load(index, src, dst):
        return pltpu.make_async_copy(src, dst, load_sem.at[index])

    depth = hid.shape[1]
    cut = depth // K_CUTS
    cuts = [slice(index * cut, (index + 1) * cut) for index in range(K_CUTS)]
    loads = []
    for index, part in enumerate(cuts):
        loads += [
            load(index, hidden_hbm.at[:, part], hid.at[:, part]),
            load(index, k1_hbm.at[part], wk1.at[part]),
            load(index, k2_hbm.at[part], wk2.at[part]),
        ]
    loads += [
        load(K_CUTS, v_hbm, wv),
        load(K_CUTS + 1, q1_hbm, wq1),
        load(K_CUTS + 1, q2_hbm, wq2),
        load(K_CUTS + 2, wo_hbm, wo.at[core]),
        load(K_CUTS + 3, lam_hbm, lam_ref),
        load(K_CUTS + 4, gain_hbm, gain_ref),
    ]
    for item in loads:
        item.start()

    def loaded(index, ref):
        pltpu.make_async_copy(ref, ref, load_sem.at[index]).wait()

    barrier = pltpu.get_barrier_semaphore()

    def greet(index, tp_index):
        pl.semaphore_signal(barrier, inc=1, device_id=(index, tp_index), device_id_type=MESH)

    def owner(index):
        return index * PLANE + mine, y

    for step in range(1, groups):
        greet(*owner(lax.rem(plane + step, groups)))
    pl.when(away)(lambda: greet(*owner(plane)))
    greet(me, 1 - core)
    greet(me + 1 - 2 * x, core)

    def send(src, dst, recv_sem, index, tp_index, send_sem=None):
        return pltpu.make_async_remote_copy(
            src_ref=src,
            dst_ref=dst,
            send_sem=sent if send_sem is None else send_sem,
            recv_sem=recv_sem,
            device_id=(index, tp_index),
            device_id_type=MESH,
        )

    def arrived(ref, recv_sem):
        pltpu.make_async_copy(ref, ref, recv_sem).wait()

    half = groups // 2
    upper = plane >= half
    lower = jnp.logical_not(upper)
    base = jnp.where(upper, half, 0)
    swapped = lax.rem(plane, half) == 0

    def from_plane(step):
        if step < half:
            return base + lax.rem(plane + step, half)
        return (half - base) + jnp.where(swapped, groups - 1 - step, step - half)

    def project(weight_ref):
        return jnp.dot(hid[...], weight_ref[...], preferred_element_type=jnp.float32)

    def joined(first, second, store):
        for head in range(groups):
            cut = slice(head * qk, (head + 1) * qk)
            store(head, jnp.concatenate((first[:, cut], second[:, cut]), axis=1))

    def z_copy(kind, step):
        target = from_plane(step)
        out, full, recvs = {
            "k": (k_out, k_all.at[me], zk_recv),
            "v": (v_out, v_all.at[me], zv_recv),
            "q": (q_out, q_all.at[plane], q_recv),
        }[kind]
        return send(
            out.at[target],
            full,
            recvs.at[plane],
            *owner(target),
        )

    def z_start(*items):
        for kind, step in items:
            z_copy(kind, step).start()

    def perform(items):
        for item in items:
            kind, step = item[0], int(item[1])
            if kind in "kvq":
                z_copy(kind, step).start()
            else:
                {"z": forward, "r": relay, "w": ready, "a": ready_q}[kind](step)

    places = [
        jnp.logical_and(plane == index, place) for index in range(groups) for place in (home, away)
    ]

    def moment(name):
        texts = [order.get(name, "") for order in ORDER]
        lists = [[text[i : i + 2] for i in range(0, len(text), 2)] for text in texts]
        if all(items == lists[0] for items in lists):
            perform(lists[0])
            return
        for items in dict.fromkeys(map(tuple, lists)):
            if items:
                place = functools.reduce(
                    jnp.logical_or, [p for p, other in zip(places, lists) if tuple(other) == items]
                )
                pl.when(place)(lambda items=items: perform(items))

    def x_block(step):
        return from_plane(step) * PLANE + mine + 1 - 2 * x

    def y_block(step):
        return from_plane(step) * PLANE + mine + 2 - 4 * core

    def to_x(slot, recvs, step):
        return send(slot, slot, recvs.at[step], me + 1 - 2 * x, core)

    def to_y(slot, step):
        return send(slot, slot, y_recv.at[step], me, 1 - core)

    def spread_k(step):
        slot = k_all.at[from_plane(step) * PLANE + mine]
        return (to_x(slot, xk_recv, step), to_y(slot, step))

    def spread_v(step):
        slot = v_all.at[from_plane(step) * PLANE + mine]
        return (to_x(slot, xv_recv, step), to_y(slot, step))

    def relay_k(step):
        return (to_y(k_all.at[x_block(step)], step),)

    def relay_v(step):
        return (to_y(v_all.at[x_block(step)], step),)

    def start(copies):
        for copy in copies:
            copy.start()

    def forward(step):
        source = from_plane(step)
        with scope(f"zk#s={step}"):
            arrived(k_all.at[source * PLANE + mine], zk_recv.at[source])
        start(spread_k(step))
        with scope(f"zv#s={step}"):
            arrived(v_all.at[source * PLANE + mine], zv_recv.at[source])
        start(spread_v(step))

    def relay(step):
        with scope(f"rk#s={step}"):
            arrived(k_all.at[x_block(step)], xk_recv.at[step])
        start(relay_k(step))
        with scope(f"rv#s={step}"):
            arrived(v_all.at[x_block(step)], xv_recv.at[step])
        start(relay_v(step))

    def ready(step):
        with scope(f"ready#s={step}"):
            arrived(k_all.at[pl.ds(0, 4)], y_recv.at[step])

    def ready_q(step):
        with scope(f"q#s={step}"):
            slot = q_all.at[from_plane(step)]
            arrived(slot, q_recv.at[from_plane(step)])

    with scope("p_k"):
        first = second = None
        for index, part in enumerate(cuts):
            with scope(f"w_k#{index}"):
                loaded(index, wv.at[pl.ds(0, cut * (rows + 2 * wk1.shape[1]) // wv.shape[1])])
            more = [
                jnp.dot(hid[:, part], weight[part], preferred_element_type=jnp.float32)
                for weight in (wk1, wk2)
            ]
            first = more[0] if first is None else first + more[0]
            second = more[1] if second is None else second + more[1]
        first = first.astype(jnp.bfloat16)
        second = second.astype(jnp.bfloat16)

        def put_k(head, value):
            k_out[head] = value

        joined(first, second, put_k)

        @pl.when(home)
        def _():
            k_all[me] = k_out[plane]

    with scope("barrier"):
        pl.semaphore_wait(barrier, groups - 1 + 2 + jnp.where(away, 1, 0))
    pl.when(home)(lambda: start(spread_k(0)))
    moment("k")
    with scope("w_v"):
        loaded(K_CUTS, wv)
    with scope("p_v"):
        value = project(wv).astype(jnp.bfloat16)
        for head in range(groups):
            v_out[head] = value[:, head * head_v : (head + 1) * head_v]

        @pl.when(home)
        def _():
            v_all[me] = v_out[plane]

    pl.when(home)(lambda: start(spread_v(0)))
    moment("v")
    with scope("w_q"):
        loaded(K_CUTS + 1, wv)
    with scope("p_q"):
        first = (project(wq1) * score_scale).astype(jnp.bfloat16)
        second = (project(wq2) * score_scale).astype(jnp.bfloat16)

        def put_q(head, value):
            q_out[head] = value

        joined(first, second, put_q)

        @pl.when(home)
        def _():
            q_all[plane] = q_out[plane]

    moment("q")
    loaded(K_CUTS + 2, wo.at[core])
    wo_copy = send(wo.at[core], wo.at[core], wo_recv, me, 1 - core, wo_sent)
    wo_copy.start()
    loads[-2].wait()
    loads[-1].wait()
    for head in range(groups):
        lam_all[core, head] = jnp.full(lam_all.shape[2:], lam_ref[head], jnp.float32)
    lam_copy = send(lam_all.at[core], lam_all.at[core], lam_recv, me, 1 - core, lam_sent)
    lam_copy.start()

    tile = ROW_TILE
    tiles = rows // tile
    lane = lax.broadcasted_iota(jnp.int32, (tile, width), 1)

    def pair_tile(group, key_group, part, diagonal, span):
        chunk = span * rows
        begin_row = pl.multiple_of(part * tile, tile)
        queries = q_all[group, pl.ds(begin_row, tile), :]
        zero = jnp.zeros_like(queries)
        both = jnp.concatenate(
            (jnp.where(lane < qk, queries, zero), jnp.where(lane >= qk, queries, zero)), axis=0
        )
        keys = k_all[pl.ds(key_group * PLANE, span)].reshape(chunk, width)
        values = v_all[pl.ds(key_group * PLANE, span)].reshape(chunk, head_v)
        scores = lax.dot_general(
            both, keys, (((1,), (1,)), ((), ())), preferred_element_type=jnp.float32
        )
        cuts = [scores[:, c * LANES : (c + 1) * LANES] for c in range(chunk // LANES)]
        if diagonal:
            row = lax.rem(lax.broadcasted_iota(jnp.int32, (2 * tile, LANES), 0), tile)
            slack = (
                mine * rows
                + begin_row
                + row
                - lax.broadcasted_iota(jnp.int32, (2 * tile, LANES), 1)
            )
            cuts = [jnp.where(slack >= c * LANES, cut, masked_score) for c, cut in enumerate(cuts)]
        highest = cuts[0]
        for cut in cuts[1:]:
            highest = jnp.maximum(highest, cut)
        running_max = max_all[group, part]
        new_max = jnp.maximum(
            running_max,
            jnp.broadcast_to(jnp.max(highest, axis=-1, keepdims=True), highest.shape),
        )
        rescale = jnp.exp2(running_max - new_max)
        weights = [jnp.exp2(cut - new_max) for cut in cuts]
        new_sum = weights[0]
        for weight in weights[1:]:
            new_sum = new_sum + weight
        accum = jnp.dot(
            jnp.concatenate([weight.astype(jnp.bfloat16) for weight in weights], axis=1),
            values,
            preferred_element_type=jnp.float32,
        )
        max_all[group, part] = new_max
        sum_all[group, part] = sum_all[group, part] * rescale + new_sum
        acc_all[group, part] = acc_all[group, part] * rescale + accum

    def pair(group, key_group, diagonal, span=PLANE):
        if not COMPUTE:
            return
        with scope("pair_d" if diagonal else "pair"):
            lax.fori_loop(
                0, tiles, lambda t, c: (pair_tile(group, key_group, t, diagonal, span), c)[1], 0
            )

    def meet(step, earlier):
        one, other = from_plane(step), from_plane(earlier)
        pair(jnp.maximum(one, other), jnp.minimum(one, other), False)

    def normed_copy(group):
        return send(
            n_out.at[group],
            n_all.at[y, plane],
            n_recv.at[plane],
            *owner(group),
        )

    def partner_copy(head):
        slot = n_all.at[core, head]
        return send(slot, slot, r_recv.at[head // half], me, 1 - core)

    gain = gain_ref[...]

    def finish(step):
        group = from_plane(step)
        if not COMPUTE:
            return

        def finish_tile(part, _):
            begin_row = pl.multiple_of(part * tile, tile)
            heads_out = acc_all[group, part] / jnp.sum(
                sum_all[group, part], axis=-1, keepdims=True
            )
            mixed = heads_out[:tile] - lam_all[y, plane][:1] * heads_out[tile:]
            scale_rows = lax.rsqrt(jnp.mean(mixed * mixed, axis=-1, keepdims=True) + epsilon)
            normed = (mixed * scale_rows * gain).astype(jnp.bfloat16)
            n_out[group, pl.ds(begin_row, tile), :] = normed
            return 0

        lax.fori_loop(0, tiles, finish_tile, 0)

    def deliver(step):
        finish(step)
        group = from_plane(step)
        if step == 0:

            @pl.when(home)
            def _():
                n_all[core, plane] = n_out[plane]
                partner_copy(plane).start()

            @pl.when(away)
            def _():
                normed_copy(group).start()

        else:
            normed_copy(group).start()

    max_all[...] = jnp.full(max_all.shape, masked_score, jnp.float32)
    sum_all[...] = jnp.zeros(sum_all.shape, jnp.float32)
    acc_all[...] = jnp.zeros(acc_all.shape, jnp.float32)

    def diagonal(step):
        group = from_plane(step)
        pl.when(core == 0)(lambda: pair(group, group, True, PLANE // 2))
        pl.when(core != 0)(lambda: pair(group, group, True))

    moment("0")
    arrived(lam_all.at[1 - core], lam_recv)
    diagonal(0)
    moment("1")
    meet(1, 0)
    diagonal(1)

    @pl.when(lower)
    def _():
        deliver(1)
        deliver(0)

    moment("2")
    meet(2, 0)
    moment("2a")
    meet(2, 1)
    moment("2b")
    diagonal(2)

    @pl.when(jnp.logical_not(swapped))
    def _():
        deliver(2)

    moment("3")

    @pl.when(jnp.logical_not(swapped))
    def _():
        meet(3, 2)

    moment("3a")

    @pl.when(lower)
    def _():
        meet(3, 0)
        meet(3, 1)

    moment("4")

    @pl.when(jnp.logical_and(swapped, lower))
    def _():
        meet(3, 2)
        deliver(2)

    diagonal(3)
    deliver(3)

    @pl.when(jnp.logical_and(swapped, upper))
    def _():
        meet(3, 2)
        deliver(2)

    @pl.when(upper)
    def _():
        meet(3, 1)
        deliver(1)
        meet(3, 0)
        deliver(0)

    def collect(head):
        @pl.when(jnp.logical_or(plane != head, away))
        def _():
            slot = n_all.at[core, head]
            with scope(f"n#h={head}"):
                arrived(slot, n_recv.at[head])
            partner_copy(head).start()

    def out_part(tp_index, first, last):
        heads = slice(first * head_v, (first + half) * head_v)
        with scope(f"out#f={first}"):
            normed = jnp.concatenate(
                [n_all[tp_index, head] for head in range(first, first + half)], axis=1
            )

            def out_tile(index, _):
                columns = pl.ds(pl.multiple_of(index * OUT_TILE, OUT_TILE), OUT_TILE)
                part = jnp.dot(
                    normed, wo[tp_index, heads, columns], preferred_element_type=jnp.float32
                )
                if last is not None:
                    part = part + out_acc[:, columns]
                if last:
                    out_ref[:, columns] = part.astype(jnp.bfloat16)
                else:
                    out_acc[:, columns] = part
                return 0

            lax.fori_loop(0, out_ref.shape[1] // OUT_TILE, out_tile, 0)

    for first in range(0, groups, half):
        for head in range(first, first + half):
            collect(head)
        out_part(core, first, None if first == 0 else False)
    arrived(wo.at[1 - core], wo_recv)
    for first in range(0, groups, half):
        with scope(f"rrecv#f={first}"):
            arrived(n_all.at[1 - core, pl.ds(first, half)], r_recv.at[first // half])
        out_part(1 - core, first, first + half == groups)

    with scope("drain"):
        wo_copy.wait_send()
        lam_copy.wait_send()
        unit = rows * width // (2 * wo.shape[2])
        for place, extra in ((home, 0), (away, 4)):
            blocks = (groups - 1) * 4 + 6 * groups + groups + extra

            @pl.when(place)
            def _():
                arrived(wo.at[:, pl.ds(0, blocks * unit)], sent)


K_CUTS = 4
COMPUTE = True
ORDER = (
    {"k": "k1", "v": "v1k2v2k3v3", "q": "q1", "0": "r0z1w0", "1": "z2r1w1q2q3a1", "2": "z3r2a2", "2b": "w2r3", "3": "a3", "4": "w3"},
    {"k": "k0", "v": "v0k1v1k2v2k3v3", "q": "q0q1", "0": "z0z1r0w0a0", "1": "z2r1w1q2q3a1", "2": "z3r2a2", "2b": "w2r3", "3": "a3", "4": "w3"},
    {"k": "k1k2", "v": "v1v2k3v3", "q": "q1q2q3", "0": "r0z1w0", "1": "z2r1z3w1a1", "2": "r2a2", "2b": "w2r3", "3": "a3", "4": "w3"},
    {"k": "k0", "v": "v0k1v1k2v2k3v3", "q": "q0q1q2q3", "0": "z0z1r0w0a0", "1": "z2r1z3w1a1", "2": "r2a2", "2b": "w2r3", "3": "a3", "4": "w3"},
    {"k": "k1k2", "v": "v1v2k3v3", "q": "q1q2q3", "0": "r0z1w0", "1": "z2r1z3w1a1", "2": "r2w2", "2b": "r3a2", "3": "a3", "4": "w3"},
    {"k": "k0", "v": "v0k1v1k2v2k3v3", "q": "q0q1q2q3", "0": "z0z1r0w0a0", "1": "z2r1z3w1a1", "2": "r2w2", "2b": "r3a2", "3": "a3", "4": "w3"},
    {"k": "k1", "v": "v1k2v2k3v3", "q": "q1", "0": "r0z1w0", "1": "z2r1w1q2q3a1", "2": "z3r2w2", "2b": "r3a2", "3": "a3", "4": "w3"},
    {"k": "k0", "v": "v0k1v1k2v2k3v3", "q": "q0q1", "0": "z0z1r0w0a0", "1": "z2r1w1q2q3a1", "2": "z3r2w2", "2b": "r3a2", "3": "a3", "4": "w3"},
)


def fused_shards(
    hidden_in, query_one, query_two, key_one, key_two, value_proj, lambdas, norm_gain, out_proj
):
    groups = lambdas.shape[0]
    rows, depth = hidden_in.shape
    head_qk = query_one.shape[1] // groups
    head_v = value_proj.shape[1] // groups
    width = 2 * head_qk
    blocks = groups * PLANE
    columns = out_proj.shape[1]
    score_scale = 1.75 * head_qk ** (-0.5) * math.log2(math.e)
    bf16 = jnp.bfloat16
    dma = pltpu.SemaphoreType.DMA
    hbm = pl.BlockSpec(memory_space=pltpu.HBM)
    vmem = pl.BlockSpec(memory_space=pltpu.VMEM)

    def body(*refs):
        fused_kernel(groups, score_scale, *refs)

    return pl.pallas_call(
        body,
        name="fused_attention",
        out_shape=jax.ShapeDtypeStruct((rows, columns), bf16),
        in_specs=[hbm] * 9,
        out_specs=vmem,
        scratch_shapes=[
            pltpu.VMEM(hidden_in.shape, bf16),
            pltpu.VMEM(query_one.shape, bf16),
            pltpu.VMEM(query_two.shape, bf16),
            pltpu.VMEM(key_one.shape, bf16),
            pltpu.VMEM(key_two.shape, bf16),
            pltpu.VMEM(value_proj.shape, bf16),
            pltpu.VMEM((2,) + out_proj.shape, bf16),
            pltpu.SMEM(lambdas.shape, jnp.float32),
            pltpu.VMEM((2, groups, 8, head_v), jnp.float32),
            pltpu.VMEM((1, head_v), jnp.float32),
            pltpu.VMEM((groups, rows, width), bf16),
            pltpu.VMEM((groups, rows, head_v), bf16),
            pltpu.VMEM((groups, rows, width), bf16),
            pltpu.VMEM((blocks, rows, width), bf16),
            pltpu.VMEM((blocks, rows, head_v), bf16),
            pltpu.VMEM((groups, rows, width), bf16),
            pltpu.VMEM((groups, rows, head_v), bf16),
            pltpu.VMEM((2, groups, rows, head_v), bf16),
            pltpu.VMEM((groups, rows // ROW_TILE, 2 * ROW_TILE, LANES), jnp.float32),
            pltpu.VMEM((groups, rows // ROW_TILE, 2 * ROW_TILE, LANES), jnp.float32),
            pltpu.VMEM((groups, rows // ROW_TILE, 2 * ROW_TILE, head_v), jnp.float32),
            pltpu.VMEM((rows, columns), jnp.float32),
            dma((K_CUTS + 5,)),
            dma,
            dma,
            dma,
            dma,
            dma,
        ]
        + [dma((groups,))] * 7
        + [dma((2,))],
        compiler_params=pltpu.CompilerParams(
            collective_id=0, has_side_effects=True, vmem_limit_bytes=VMEM_LIMIT
        ),
    )(
        *(
            pltpu.with_memory_space_constraint(item, pltpu.HBM)
            for item in (
                hidden_in,
                query_one,
                query_two,
                key_one,
                key_two,
                value_proj,
                lambdas,
                norm_gain.reshape(1, head_v),
                out_proj,
            )
        )
    )


VMEM_LIMIT = 48 * 1024 * 1024


def solution(mesh):
    placed = (
        P("sp", None),
        P(None, "tp"),
        P(None, "tp"),
        P(None, "tp"),
        P(None, "tp"),
        P(None, "tp"),
        P("tp"),
        P(),
        P("tp", None),
    )

    def body(*args):
        groups = args[6].shape[0]
        split = groups * PLANE == mesh.shape["sp"] and mesh.shape["tp"] == 2
        return (fused_shards if split else shards)(*args)

    return jax.shard_map(
        body, mesh=mesh, in_specs=placed, out_specs=P("sp", None), check_vma=False
    )
```

```python
import functools
import math

import jax
import jax.numpy as jnp
from jax import lax
from jax.experimental import pallas as pl
from jax.experimental.pallas import tpu as pltpu
from jax.sharding import PartitionSpec as P

epsilon = 1e-06
masked_score = -1e30


def shards(
    hidden_in, query_one, query_two, key_one, key_two, value_proj, lambdas, norm_gain, out_proj
):
    heads_dev = lambdas.shape[0]
    head_qk = query_one.shape[1] // heads_dev
    head_v = value_proj.shape[1] // heads_dev
    width_q = heads_dev * head_qk
    score_scale = 1.75 * head_qk ** (-0.5)
    joined = jnp.concatenate((query_one, query_two, key_one, key_two, value_proj), axis=1)
    projected = jnp.dot(hidden_in, joined, preferred_element_type=jnp.float32).astype(jnp.bfloat16)
    tok_rows = projected.shape[0]
    key_values = projected[:, 2 * width_q :]
    my_index = lax.axis_index("sp")
    offset = my_index * tok_rows
    query_sets = (projected[:, : 2 * width_q],)
    position_sets = (offset + jnp.arange(tok_rows, dtype=jnp.int32),)
    groups = []
    for query_rows, positions in zip(query_sets, position_sets):
        group_rows = query_rows.shape[0]
        query_a = query_rows[:, :width_q].reshape(group_rows, heads_dev, head_qk)
        query_b = query_rows[:, width_q:].reshape(group_rows, heads_dev, head_qk)
        groups.append((query_a, query_b, positions, positions[group_rows - 1]))

    def one_map(queries, keys, value_rows, allowed, running_max, running_sum, accum):
        scores = (
            jnp.einsum("qhd,khd->hqk", queries, keys, preferred_element_type=jnp.float32)
            * score_scale
        )
        scores = jnp.where(allowed[None], scores, masked_score)
        new_max = jnp.maximum(running_max, jnp.max(scores, axis=-1))
        rescale = jnp.exp(running_max - new_max)
        weights = jnp.where(allowed[None], jnp.exp(scores - new_max[..., None]), 0.0)
        new_sum = running_sum * rescale + jnp.sum(weights, axis=-1)
        added = jnp.einsum(
            "hqk,khe->hqe",
            weights.astype(jnp.bfloat16),
            value_rows,
            preferred_element_type=jnp.float32,
        )
        return (new_max, new_sum, accum * rescale[..., None] + added)

    def absorb(group_state, group, kblock, kstart):
        query_a, query_b, positions, last_pos = group
        block_rows = kblock.shape[0]
        k_pos = kstart + jnp.arange(block_rows, dtype=jnp.int32)
        allowed = k_pos[None, :] <= positions[:, None]
        keys_a = kblock[:, :width_q].reshape(block_rows, heads_dev, head_qk)
        keys_b = kblock[:, width_q : 2 * width_q].reshape(block_rows, heads_dev, head_qk)
        value_rows = kblock[:, 2 * width_q :].reshape(block_rows, heads_dev, head_v)
        first_map = one_map(query_a, keys_a, value_rows, allowed, *group_state[:3])
        second_map = one_map(query_b, keys_b, value_rows, allowed, *group_state[3:])
        return first_map + second_map

    group = groups[0]
    group_rows = group[0].shape[0]
    start_max = jnp.full((heads_dev, group_rows), masked_score, jnp.float32)
    start_sum = jnp.zeros((heads_dev, group_rows), jnp.float32)
    start_acc = jnp.zeros((heads_dev, group_rows, head_v), jnp.float32)
    initial_list = [(start_max, start_sum, start_acc, start_max, start_sum, start_acc)]
    initial = tuple(initial_list)
    softmax_state = initial
    kv_piece = lax.all_gather(key_values, "sp", axis=0, tiled=True)
    piece_rows = kv_piece.shape[0]
    block_rows = math.gcd(piece_rows, 512)
    block_count = piece_rows // block_rows
    stacked = kv_piece.reshape(block_count, block_rows, kv_piece.shape[1])

    def absorb_step(carried, blocks_in):
        kblock, block_index = blocks_in
        kstart = block_index * block_rows
        renewed = []
        for group, group_state in zip(groups, carried):
            renewed.append(
                lax.cond(
                    kstart <= group[3],
                    lambda inner, group=group: absorb(inner, group, kblock, kstart),
                    lambda inner: inner,
                    group_state,
                )
            )
        return (tuple(renewed), None)

    softmax_state, _ = lax.scan(
        absorb_step, softmax_state, (stacked, jnp.arange(block_count, dtype=jnp.int32))
    )
    normed_sets = []
    for group_state in softmax_state:
        out_a = group_state[2] / group_state[1][..., None]
        out_b = group_state[5] / group_state[4][..., None]
        mixed_out = out_a - lambdas[:, None, None] * out_b
        scale_rows = lax.rsqrt(jnp.mean(mixed_out * mixed_out, axis=-1, keepdims=True) + epsilon)
        normed = (mixed_out * scale_rows * norm_gain).astype(jnp.bfloat16)
        group_rows = normed.shape[1]
        normed_sets.append(jnp.transpose(normed, (1, 0, 2)).reshape(group_rows, heads_dev * head_v))
    normed_all = normed_sets[0]
    partial_value = jnp.dot(normed_all, out_proj, preferred_element_type=jnp.float32)
    result = lax.psum(partial_value.astype(jnp.bfloat16), "tp")
    return result


MESH = pl.DeviceIdType.MESH
PLANE = 4
ROW_TILE = 256
OUT_TILE = 2048
LANES = 128


def fused_kernel(
    groups,
    score_scale,
    hidden_hbm,
    q1_hbm,
    q2_hbm,
    k1_hbm,
    k2_hbm,
    v_hbm,
    lam_hbm,
    gain_hbm,
    wo_hbm,
    out_ref,
    hid,
    wq1,
    wq2,
    wk1,
    wk2,
    wv,
    wo,
    lam_ref,
    lam_all,
    gain_ref,
    k_out,
    v_out,
    q_out,
    k_all,
    v_all,
    q_all,
    n_out,
    n_all,
    max_all,
    sum_all,
    acc_all,
    out_acc,
    load_sem,
    sent,
    wo_sent,
    wo_recv,
    lam_sent,
    lam_recv,
    zk_recv,
    zv_recv,
    q_recv,
    xk_recv,
    xv_recv,
    y_recv,
    n_recv,
    r_recv,
):
    scope = jax.named_scope
    me = lax.axis_index("sp")
    core = lax.axis_index("tp")
    plane = me // PLANE
    spot = lax.rem(me, PLANE)
    x = lax.rem(spot, 2)
    y = spot // 2
    mine = 2 * core + x
    home = core == y
    away = core != y
    rows = hid.shape[0]
    qk = q1_hbm.shape[1] // groups
    width = 2 * qk
    head_v = v_hbm.shape[1] // groups

    def load(index, src, dst):
        return pltpu.make_async_copy(src, dst, load_sem.at[index])

    depth = hid.shape[1]
    cut = depth // K_CUTS
    cuts = [slice(index * cut, (index + 1) * cut) for index in range(K_CUTS)]
    loads = []
    for index, part in enumerate(cuts):
        loads += [
            load(index, hidden_hbm.at[:, part], hid.at[:, part]),
            load(index, k1_hbm.at[part], wk1.at[part]),
            load(index, k2_hbm.at[part], wk2.at[part]),
        ]
    loads += [
        load(K_CUTS, v_hbm, wv),
        load(K_CUTS + 1, q1_hbm, wq1),
        load(K_CUTS + 1, q2_hbm, wq2),
        load(K_CUTS + 2, wo_hbm, wo.at[core]),
        load(K_CUTS + 3, lam_hbm, lam_ref),
        load(K_CUTS + 4, gain_hbm, gain_ref),
    ]
    for item in loads:
        item.start()

    def loaded(index, ref):
        pltpu.make_async_copy(ref, ref, load_sem.at[index]).wait()

    barrier = pltpu.get_barrier_semaphore()

    def greet(index, tp_index):
        pl.semaphore_signal(barrier, inc=1, device_id=(index, tp_index), device_id_type=MESH)

    def owner(index):
        return index * PLANE + mine, y

    for step in range(1, groups):
        greet(*owner(lax.rem(plane + step, groups)))
    pl.when(away)(lambda: greet(*owner(plane)))
    greet(me, 1 - core)
    greet(me + 1 - 2 * x, core)

    def send(src, dst, recv_sem, index, tp_index, send_sem=None):
        return pltpu.make_async_remote_copy(
            src_ref=src,
            dst_ref=dst,
            send_sem=sent if send_sem is None else send_sem,
            recv_sem=recv_sem,
            device_id=(index, tp_index),
            device_id_type=MESH,
        )

    def arrived(ref, recv_sem):
        pltpu.make_async_copy(ref, ref, recv_sem).wait()

    half = groups // 2
    upper = plane >= half
    lower = jnp.logical_not(upper)
    base = jnp.where(upper, half, 0)
    swapped = lax.rem(plane, half) == 0

    def from_plane(step):
        if step < half:
            return base + lax.rem(plane + step, half)
        return (half - base) + jnp.where(swapped, groups - 1 - step, step - half)

    def project(weight_ref):
        return jnp.dot(hid[...], weight_ref[...], preferred_element_type=jnp.float32)

    def joined(first, second, store):
        for head in range(groups):
            cut = slice(head * qk, (head + 1) * qk)
            store(head, jnp.concatenate((first[:, cut], second[:, cut]), axis=1))

    def z_copy(kind, step):
        target = from_plane(step)
        out, full, recvs = {
            "k": (k_out, k_all.at[me], zk_recv),
            "v": (v_out, v_all.at[me], zv_recv),
            "q": (q_out, q_all.at[plane], q_recv),
        }[kind]
        return send(
            out.at[target],
            full,
            recvs.at[plane],
            *owner(target),
        )

    def z_start(*items):
        for kind, step in items:
            z_copy(kind, step).start()

    def perform(items):
        for item in items:
            kind, step = item[0], int(item[1])
            if kind in "kvq":
                z_copy(kind, step).start()
            else:
                {"z": forward, "r": relay, "w": ready, "a": ready_q}[kind](step)

    places = [
        jnp.logical_and(plane == index, place) for index in range(groups) for place in (home, away)
    ]

    def moment(name):
        texts = [order.get(name, "") for order in ORDER]
        lists = [[text[i : i + 2] for i in range(0, len(text), 2)] for text in texts]
        if all(items == lists[0] for items in lists):
            perform(lists[0])
            return
        for items in dict.fromkeys(map(tuple, lists)):
            if items:
                place = functools.reduce(
                    jnp.logical_or, [p for p, other in zip(places, lists) if tuple(other) == items]
                )
                pl.when(place)(lambda items=items: perform(items))

    def x_block(step):
        return from_plane(step) * PLANE + mine + 1 - 2 * x

    def y_block(step):
        return from_plane(step) * PLANE + mine + 2 - 4 * core

    def to_x(slot, recvs, step):
        return send(slot, slot, recvs.at[step], me + 1 - 2 * x, core)

    def to_y(slot, step):
        return send(slot, slot, y_recv.at[step], me, 1 - core)

    def spread_k(step):
        slot = k_all.at[from_plane(step) * PLANE + mine]
        return (to_x(slot, xk_recv, step), to_y(slot, step))

    def spread_v(step):
        slot = v_all.at[from_plane(step) * PLANE + mine]
        return (to_x(slot, xv_recv, step), to_y(slot, step))

    def relay_k(step):
        return (to_y(k_all.at[x_block(step)], step),)

    def relay_v(step):
        return (to_y(v_all.at[x_block(step)], step),)

    def start(copies):
        for copy in copies:
            copy.start()

    def forward(step):
        source = from_plane(step)
        with scope(f"zk#s={step}"):
            arrived(k_all.at[source * PLANE + mine], zk_recv.at[source])
        start(spread_k(step))
        with scope(f"zv#s={step}"):
            arrived(v_all.at[source * PLANE + mine], zv_recv.at[source])
        start(spread_v(step))

    def relay(step):
        with scope(f"rk#s={step}"):
            arrived(k_all.at[x_block(step)], xk_recv.at[step])
        start(relay_k(step))
        with scope(f"rv#s={step}"):
            arrived(v_all.at[x_block(step)], xv_recv.at[step])
        start(relay_v(step))

    def ready(step):
        with scope(f"ready#s={step}"):
            arrived(k_all.at[pl.ds(0, 4)], y_recv.at[step])

    def ready_q(step):
        with scope(f"q#s={step}"):
            slot = q_all.at[from_plane(step)]
            arrived(slot, q_recv.at[from_plane(step)])

    with scope("p_k"):
        first = second = None
        for index, part in enumerate(cuts):
            with scope(f"w_k#{index}"):
                loaded(index, wv.at[pl.ds(0, cut * (rows + 2 * wk1.shape[1]) // wv.shape[1])])
            more = [
                jnp.dot(hid[:, part], weight[part], preferred_element_type=jnp.float32)
                for weight in (wk1, wk2)
            ]
            first = more[0] if first is None else first + more[0]
            second = more[1] if second is None else second + more[1]
        first = first.astype(jnp.bfloat16)
        second = second.astype(jnp.bfloat16)

        def put_k(head, value):
            k_out[head] = value

        joined(first, second, put_k)

        @pl.when(home)
        def _():
            k_all[me] = k_out[plane]

    with scope("barrier"):
        pl.semaphore_wait(barrier, groups - 1 + 2 + jnp.where(away, 1, 0))
    pl.when(home)(lambda: start(spread_k(0)))
    moment("k")
    with scope("w_v"):
        loaded(K_CUTS, wv)
    with scope("p_v"):
        value = project(wv).astype(jnp.bfloat16)
        for head in range(groups):
            v_out[head] = value[:, head * head_v : (head + 1) * head_v]

        @pl.when(home)
        def _():
            v_all[me] = v_out[plane]

    pl.when(home)(lambda: start(spread_v(0)))
    moment("v")
    with scope("w_q"):
        loaded(K_CUTS + 1, wv)
    with scope("p_q"):
        first = (project(wq1) * score_scale).astype(jnp.bfloat16)
        second = (project(wq2) * score_scale).astype(jnp.bfloat16)

        def put_q(head, value):
            q_out[head] = value

        joined(first, second, put_q)

        @pl.when(home)
        def _():
            q_all[plane] = q_out[plane]

    moment("q")
    loaded(K_CUTS + 2, wo.at[core])
    wo_copy = send(wo.at[core], wo.at[core], wo_recv, me, 1 - core, wo_sent)
    wo_copy.start()
    loads[-2].wait()
    loads[-1].wait()
    for head in range(groups):
        lam_all[core, head] = jnp.full(lam_all.shape[2:], lam_ref[head], jnp.float32)
    lam_copy = send(lam_all.at[core], lam_all.at[core], lam_recv, me, 1 - core, lam_sent)
    lam_copy.start()

    tile = ROW_TILE
    tiles = rows // tile
    lane = lax.broadcasted_iota(jnp.int32, (tile, width), 1)

    def pair_tile(group, key_group, part, diagonal, span):
        chunk = span * rows
        begin_row = pl.multiple_of(part * tile, tile)
        queries = q_all[group, pl.ds(begin_row, tile), :]
        zero = jnp.zeros_like(queries)
        both = jnp.concatenate(
            (jnp.where(lane < qk, queries, zero), jnp.where(lane >= qk, queries, zero)), axis=0
        )
        keys = k_all[pl.ds(key_group * PLANE, span)].reshape(chunk, width)
        values = v_all[pl.ds(key_group * PLANE, span)].reshape(chunk, head_v)
        scores = lax.dot_general(
            both, keys, (((1,), (1,)), ((), ())), preferred_element_type=jnp.float32
        )
        cuts = [scores[:, c * LANES : (c + 1) * LANES] for c in range(chunk // LANES)]
        if diagonal:
            row = lax.rem(lax.broadcasted_iota(jnp.int32, (2 * tile, LANES), 0), tile)
            slack = (
                mine * rows
                + begin_row
                + row
                - lax.broadcasted_iota(jnp.int32, (2 * tile, LANES), 1)
            )
            cuts = [jnp.where(slack >= c * LANES, cut, masked_score) for c, cut in enumerate(cuts)]
        highest = cuts[0]
        for cut in cuts[1:]:
            highest = jnp.maximum(highest, cut)
        running_max = max_all[group, part]
        new_max = jnp.maximum(
            running_max,
            jnp.broadcast_to(jnp.max(highest, axis=-1, keepdims=True), highest.shape),
        )
        rescale = jnp.exp2(running_max - new_max)
        weights = [jnp.exp2(cut - new_max) for cut in cuts]
        new_sum = weights[0]
        for weight in weights[1:]:
            new_sum = new_sum + weight
        accum = jnp.dot(
            jnp.concatenate([weight.astype(jnp.bfloat16) for weight in weights], axis=1),
            values,
            preferred_element_type=jnp.float32,
        )
        max_all[group, part] = new_max
        sum_all[group, part] = sum_all[group, part] * rescale + new_sum
        acc_all[group, part] = acc_all[group, part] * rescale + accum

    def pair(group, key_group, diagonal, span=PLANE):
        if not COMPUTE:
            return
        with scope("pair_d" if diagonal else "pair"):
            lax.fori_loop(
                0, tiles, lambda t, c: (pair_tile(group, key_group, t, diagonal, span), c)[1], 0
            )

    def meet(step, earlier):
        one, other = from_plane(step), from_plane(earlier)
        pair(jnp.maximum(one, other), jnp.minimum(one, other), False)

    def normed_copy(group):
        return send(
            n_out.at[group],
            n_all.at[y, plane],
            n_recv.at[plane],
            *owner(group),
        )

    def partner_copy(head):
        slot = n_all.at[core, head]
        return send(slot, slot, r_recv.at[head // half], me, 1 - core)

    gain = gain_ref[...]

    def finish(step):
        group = from_plane(step)
        if not COMPUTE:
            return

        def finish_tile(part, _):
            begin_row = pl.multiple_of(part * tile, tile)
            heads_out = acc_all[group, part] / jnp.sum(
                sum_all[group, part], axis=-1, keepdims=True
            )
            mixed = heads_out[:tile] - lam_all[y, plane][:1] * heads_out[tile:]
            scale_rows = lax.rsqrt(jnp.mean(mixed * mixed, axis=-1, keepdims=True) + epsilon)
            normed = (mixed * scale_rows * gain).astype(jnp.bfloat16)
            n_out[group, pl.ds(begin_row, tile), :] = normed
            return 0

        lax.fori_loop(0, tiles, finish_tile, 0)

    def deliver(step):
        finish(step)
        group = from_plane(step)
        if step == 0:

            @pl.when(home)
            def _():
                n_all[core, plane] = n_out[plane]
                partner_copy(plane).start()

            @pl.when(away)
            def _():
                normed_copy(group).start()

        else:
            normed_copy(group).start()

    max_all[...] = jnp.full(max_all.shape, masked_score, jnp.float32)
    sum_all[...] = jnp.zeros(sum_all.shape, jnp.float32)
    acc_all[...] = jnp.zeros(acc_all.shape, jnp.float32)

    def diagonal(step):
        group = from_plane(step)
        for last in range(PLANE):
            pl.when(mine == last)(lambda last=last: pair(group, group, True, last + 1))

    moment("0")
    arrived(lam_all.at[1 - core], lam_recv)
    diagonal(0)
    moment("1")
    meet(1, 0)
    diagonal(1)

    @pl.when(lower)
    def _():
        deliver(1)
        deliver(0)

    moment("2")
    meet(2, 0)
    moment("2a")
    meet(2, 1)
    moment("2b")
    diagonal(2)

    @pl.when(jnp.logical_not(swapped))
    def _():
        deliver(2)

    moment("3")

    @pl.when(jnp.logical_not(swapped))
    def _():
        meet(3, 2)

    moment("3a")

    @pl.when(lower)
    def _():
        meet(3, 0)
        meet(3, 1)

    moment("4")

    @pl.when(jnp.logical_and(swapped, lower))
    def _():
        meet(3, 2)
        deliver(2)

    diagonal(3)
    deliver(3)

    @pl.when(jnp.logical_and(swapped, upper))
    def _():
        meet(3, 2)
        deliver(2)

    @pl.when(upper)
    def _():
        meet(3, 1)
        deliver(1)
        meet(3, 0)
        deliver(0)

    def collect(head):
        @pl.when(jnp.logical_or(plane != head, away))
        def _():
            slot = n_all.at[core, head]
            with scope(f"n#h={head}"):
                arrived(slot, n_recv.at[head])
            partner_copy(head).start()

    def out_part(tp_index, first, last):
        heads = slice(first * head_v, (first + half) * head_v)
        with scope(f"out#f={first}"):
            normed = jnp.concatenate(
                [n_all[tp_index, head] for head in range(first, first + half)], axis=1
            )

            def out_tile(index, _):
                columns = pl.ds(pl.multiple_of(index * OUT_TILE, OUT_TILE), OUT_TILE)
                part = jnp.dot(
                    normed, wo[tp_index, heads, columns], preferred_element_type=jnp.float32
                )
                if last is not None:
                    part = part + out_acc[:, columns]
                if last:
                    out_ref[:, columns] = part.astype(jnp.bfloat16)
                else:
                    out_acc[:, columns] = part
                return 0

            lax.fori_loop(0, out_ref.shape[1] // OUT_TILE, out_tile, 0)

    for first in range(0, groups, half):
        for head in range(first, first + half):
            collect(head)
        out_part(core, first, None if first == 0 else False)
    arrived(wo.at[1 - core], wo_recv)
    for first in range(0, groups, half):
        with scope(f"rrecv#f={first}"):
            arrived(n_all.at[1 - core, pl.ds(first, half)], r_recv.at[first // half])
        out_part(1 - core, first, first + half == groups)

    with scope("drain"):
        wo_copy.wait_send()
        lam_copy.wait_send()
        unit = rows * width // (2 * wo.shape[2])
        for place, extra in ((home, 0), (away, 4)):
            blocks = (groups - 1) * 4 + 6 * groups + groups + extra

            @pl.when(place)
            def _():
                arrived(wo.at[:, pl.ds(0, blocks * unit)], sent)


K_CUTS = 4
COMPUTE = True
ORDER = (
    {"k": "k1", "v": "v1k2v2k3v3", "q": "q1", "0": "r0z1w0", "1": "z2r1w1q2q3a1", "2": "z3r2a2", "2b": "w2r3", "3": "a3", "4": "w3"},
    {"k": "k0", "v": "v0k1v1k2v2k3v3", "q": "q0q1", "0": "z0z1r0w0a0", "1": "z2r1w1q2q3a1", "2": "z3r2a2", "2b": "w2r3", "3": "a3", "4": "w3"},
    {"k": "k1k2", "v": "v1v2k3v3", "q": "q1q2q3", "0": "r0z1w0", "1": "z2r1z3w1a1", "2": "r2a2", "2b": "w2r3", "3": "a3", "4": "w3"},
    {"k": "k0", "v": "v0k1v1k2v2k3v3", "q": "q0q1q2q3", "0": "z0z1r0w0a0", "1": "z2r1z3w1a1", "2": "r2a2", "2b": "w2r3", "3": "a3", "4": "w3"},
    {"k": "k1k2", "v": "v1v2k3v3", "q": "q1q2q3", "0": "r0z1w0", "1": "z2r1z3w1a1", "2": "r2w2", "2b": "r3a2", "3": "a3", "4": "w3"},
    {"k": "k0", "v": "v0k1v1k2v2k3v3", "q": "q0q1q2q3", "0": "z0z1r0w0a0", "1": "z2r1z3w1a1", "2": "r2w2", "2b": "r3a2", "3": "a3", "4": "w3"},
    {"k": "k1", "v": "v1k2v2k3v3", "q": "q1", "0": "r0z1w0", "1": "z2r1w1q2q3a1", "2": "z3r2w2", "2b": "r3a2", "3": "a3", "4": "w3"},
    {"k": "k0", "v": "v0k1v1k2v2k3v3", "q": "q0q1", "0": "z0z1r0w0a0", "1": "z2r1w1q2q3a1", "2": "z3r2w2", "2b": "r3a2", "3": "a3", "4": "w3"},
)


def fused_shards(
    hidden_in, query_one, query_two, key_one, key_two, value_proj, lambdas, norm_gain, out_proj
):
    groups = lambdas.shape[0]
    rows, depth = hidden_in.shape
    head_qk = query_one.shape[1] // groups
    head_v = value_proj.shape[1] // groups
    width = 2 * head_qk
    blocks = groups * PLANE
    columns = out_proj.shape[1]
    score_scale = 1.75 * head_qk ** (-0.5) * math.log2(math.e)
    bf16 = jnp.bfloat16
    dma = pltpu.SemaphoreType.DMA
    hbm = pl.BlockSpec(memory_space=pltpu.HBM)
    vmem = pl.BlockSpec(memory_space=pltpu.VMEM)

    def body(*refs):
        fused_kernel(groups, score_scale, *refs)

    return pl.pallas_call(
        body,
        name="fused_attention",
        out_shape=jax.ShapeDtypeStruct((rows, columns), bf16),
        in_specs=[hbm] * 9,
        out_specs=vmem,
        scratch_shapes=[
            pltpu.VMEM(hidden_in.shape, bf16),
            pltpu.VMEM(query_one.shape, bf16),
            pltpu.VMEM(query_two.shape, bf16),
            pltpu.VMEM(key_one.shape, bf16),
            pltpu.VMEM(key_two.shape, bf16),
            pltpu.VMEM(value_proj.shape, bf16),
            pltpu.VMEM((2,) + out_proj.shape, bf16),
            pltpu.SMEM(lambdas.shape, jnp.float32),
            pltpu.VMEM((2, groups, 8, head_v), jnp.float32),
            pltpu.VMEM((1, head_v), jnp.float32),
            pltpu.VMEM((groups, rows, width), bf16),
            pltpu.VMEM((groups, rows, head_v), bf16),
            pltpu.VMEM((groups, rows, width), bf16),
            pltpu.VMEM((blocks, rows, width), bf16),
            pltpu.VMEM((blocks, rows, head_v), bf16),
            pltpu.VMEM((groups, rows, width), bf16),
            pltpu.VMEM((groups, rows, head_v), bf16),
            pltpu.VMEM((2, groups, rows, head_v), bf16),
            pltpu.VMEM((groups, rows // ROW_TILE, 2 * ROW_TILE, LANES), jnp.float32),
            pltpu.VMEM((groups, rows // ROW_TILE, 2 * ROW_TILE, LANES), jnp.float32),
            pltpu.VMEM((groups, rows // ROW_TILE, 2 * ROW_TILE, head_v), jnp.float32),
            pltpu.VMEM((rows, columns), jnp.float32),
            dma((K_CUTS + 5,)),
            dma,
            dma,
            dma,
            dma,
            dma,
        ]
        + [dma((groups,))] * 7
        + [dma((2,))],
        compiler_params=pltpu.CompilerParams(
            collective_id=0, has_side_effects=True, vmem_limit_bytes=VMEM_LIMIT
        ),
    )(
        *(
            pltpu.with_memory_space_constraint(item, pltpu.HBM)
            for item in (
                hidden_in,
                query_one,
                query_two,
                key_one,
                key_two,
                value_proj,
                lambdas,
                norm_gain.reshape(1, head_v),
                out_proj,
            )
        )
    )


VMEM_LIMIT = 48 * 1024 * 1024


def solution(mesh):
    placed = (
        P("sp", None),
        P(None, "tp"),
        P(None, "tp"),
        P(None, "tp"),
        P(None, "tp"),
        P(None, "tp"),
        P("tp"),
        P(),
        P("tp", None),
    )

    def body(*args):
        groups = args[6].shape[0]
        split = groups * PLANE == mesh.shape["sp"] and mesh.shape["tp"] == 2
        return (fused_shards if split else shards)(*args)

    return jax.shard_map(
        body, mesh=mesh, in_specs=placed, out_specs=P("sp", None), check_vma=False
    )
```
